32 devices in a mesh: rep: 4 (over z), fs: 2 (over y), tp: 4 (over x, core).
Axes of the slice: x: 2, y: 2, z: 4, core: 2. Of those that a mesh axis runs over, the one named last changes fastest.
Arguments:
- tokens: bfloat16 [1536, 2048], P('rep', ('fs', 'tp')), may hold values from -6 to 6
- cotangent: bfloat16 [1536, 2048], P('rep', ('fs', 'tp')), may hold values from -6 to 6
- gain: float32 [2048], replicated, may hold values from 0.1 to 1.9
- w_gate: bfloat16 [5376, 2048], P(('fs', 'tp')), may hold values from -0.125 to 0.125
- w_up: bfloat16 [5376, 2048], P(('fs', 'tp')), may hold values from -0.125 to 0.125
- w_down: bfloat16 [5376, 2048], P(('fs', 'tp')), may hold values from -0.078125 to 0.078125
Outputs:
- grad_input: bfloat16 [1536, 2048], P('rep', ('fs', 'tp'))
- grad_gain: float32 [2048], P(('fs', 'tp'))
- grad_gate: float32 [5376, 2048], P(('fs', 'tp'))
- grad_up: float32 [5376, 2048], P(('fs', 'tp'))
- grad_down: float32 [5376, 2048], P(('fs', 'tp'))
The draws below stay inside these ranges and needn't reach their ends.
All inputs are finite; a program needn't handle non-finite values.
Results may differ from the reference program's by a relative error of at most 0.006.
Values may be sent and summed in bfloat16 or wider, within the bound.
A program may use at most 128 MiB of HBM per device.

```python
import jax
import jax.numpy as jnp
from jax import lax

D = 2048
FF = 5376
TOKENS = 1536


def raised(array, key, source, target, parts, factor):
    def block_of(axis_at):
        return (jnp.arange(array.shape[axis_at]) // (array.shape[axis_at] // parts)).reshape((-1,) + (1,) * (array.ndim - 1 - axis_at))

    one_side = jax.random.permutation(key, parts)[block_of(target)]
    second = (block_of(target) + parts // 2) % parts
    return jnp.where((block_of(source) == one_side) | (block_of(source) == second), factor * array, array)


def block_scale(key, extent, pieces, least, top_value):
    loudness = 1.0
    for axis_at, parts in pieces:
        steps = jax.random.uniform(jax.random.fold_in(jax.random.fold_in(key, 6), axis_at), (parts,), jnp.float32, least / len(pieces), top_value / len(pieces))
        loudness = loudness * jnp.repeat(jnp.exp(steps), extent[axis_at] // parts).reshape((-1,) + (1,) * (len(extent) - 1 - axis_at))
    return loudness


def bell_draw(stream_key, dims, width, reach, pieces=(), held_as=jnp.bfloat16):
    level = block_scale(stream_key, dims, pieces, -0.22, 0.18) if pieces else 1.0
    values = jax.random.normal(stream_key, dims, jnp.float32) * width * level
    return jnp.minimum(jnp.maximum(values, -reach), reach).astype(held_as)


def noise_with(stream_key, dims, width, reach, pieces, heavy, kind=jnp.bfloat16):
    drawn = width * jax.random.normal(stream_key, dims, jnp.float32)
    if pieces:
        drawn = drawn * block_scale(stream_key, dims, pieces, -0.22, 0.18)
    return jnp.clip(raised(drawn, jax.random.fold_in(stream_key, 3), *heavy), -reach, reach).astype(kind)


def setup_inputs(seed: int = 0) -> dict:
    streams_of = jax.random.split(jax.random.key(seed), 7)
    tokens = bell_draw(streams_of[0], (TOKENS, D), 1.0, 6.0, ((0, 4), (1, 8)))
    cotangent = noise_with(streams_of[1], (TOKENS, D), 1.0, 6.0, ((0, 4), (1, 8)), (0, 1, 8, 2.0))
    gain = jnp.clip(1.0 + 0.18 * jax.random.normal(streams_of[2], (D,), jnp.float32), 0.1, 1.9)
    w_gate = bell_draw(streams_of[3], (FF, D), D ** -0.5, 0.125, ((0, 8),))
    w_up = bell_draw(streams_of[4], (FF, D), D ** -0.5, 0.125, ((0, 8),))
    w_down = bell_draw(streams_of[5], (FF, D), FF ** -0.5, 0.078125, ((0, 8),))
    return {"tokens": tokens, "cotangent": cotangent, "gain": gain, "w_gate": w_gate, "w_up": w_up, "w_down": w_down}


EPS = 1e-06

def reference(tokens, cotangent, gain, w_gate, w_up, w_down):
    xf = tokens.astype(jnp.float32)
    inv_rms = lax.rsqrt(lax.optimization_barrier(jnp.mean(xf * xf, axis=1, keepdims=True)) + EPS)
    unit = xf * inv_rms
    normed = (unit * gain).astype(jnp.bfloat16)
    gate = jnp.dot(normed, w_gate.T, preferred_element_type=jnp.float32)
    up = jnp.dot(normed, w_up.T, preferred_element_type=jnp.float32)
    sig = jax.nn.sigmoid(gate)
    active = gate * sig
    hidden = (active * up).astype(jnp.bfloat16)
    d_hidden = 0.5 * jnp.dot(cotangent, w_down.T, preferred_element_type=jnp.float32)
    d_gate = (d_hidden * up * sig * (1.0 + gate * (1.0 - sig))).astype(jnp.bfloat16)
    d_up = (d_hidden * active).astype(jnp.bfloat16)
    grad_down = 0.5 * jnp.dot(hidden.T, cotangent, preferred_element_type=jnp.float32)
    grad_gate = jnp.dot(d_gate.T, normed, preferred_element_type=jnp.float32)
    grad_up = jnp.dot(d_up.T, normed, preferred_element_type=jnp.float32)
    d_normed = jnp.dot(d_gate, w_gate, preferred_element_type=jnp.float32) + jnp.dot(d_up, w_up, preferred_element_type=jnp.float32)
    grad_gain = lax.optimization_barrier(jnp.sum(unit * d_normed, axis=0))
    d_unit = d_normed * gain
    row_mean = lax.optimization_barrier(jnp.mean(unit * d_unit, axis=1, keepdims=True))
    grad_input = (cotangent.astype(jnp.float32) + inv_rms * (d_unit - unit * row_mean)).astype(jnp.bfloat16)
    return (grad_input, grad_gain, grad_gate, grad_up, grad_down)
```

```python
import functools

import jax
import jax.numpy as jnp
from jax import lax
from jax.experimental import pallas as pl
from jax.experimental.pallas import tpu as pltpu
from jax.sharding import PartitionSpec as P

EPS = 1e-06
PLANE = ("fs", "tp")


def right_product(left, weight):
    return lax.dot_general(
        left, weight, (((1,), (1,)), ((), ())), preferred_element_type=jnp.float32
    )


def left_product(left, right):
    return lax.dot_general(
        left, right, (((0,), (0,)), ((), ())), preferred_element_type=jnp.float32
    )


def normalise(x, gain):
    xf = x.astype(jnp.float32)
    inv_rms = lax.rsqrt(jnp.mean(xf * xf, axis=1, keepdims=True) + EPS)
    return inv_rms, (xf * inv_rms * gain).astype(jnp.bfloat16)


def hidden_grads(normed, dy, w_gate, w_up, w_down):
    gate = right_product(normed, w_gate)
    up = right_product(normed, w_up)
    sig = jax.nn.sigmoid(gate)
    active = gate * sig
    hidden = (active * up).astype(jnp.bfloat16)
    d_hidden = 0.5 * right_product(dy, w_down)
    d_gate = (d_hidden * up * sig * (1.0 + gate * (1.0 - sig))).astype(jnp.bfloat16)
    d_up = (d_hidden * active).astype(jnp.bfloat16)
    return hidden, d_gate, d_up


def hidden_sum(d_gate, d_up, w_gate, w_up):
    return jnp.dot(d_gate, w_gate, preferred_element_type=jnp.float32) + jnp.dot(
        d_up, w_up, preferred_element_type=jnp.float32
    )


def axis_sums(rows_part, gain_part):
    return lax.psum(rows_part, PLANE), lax.psum(gain_part, "rep")


def input_grads(tokens, cotangent, gain, inv_rms, partial_value, sums):
    width = partial_value.shape[1]
    summed = lax.psum_scatter(
        partial_value, PLANE, scatter_dimension=1, tiled=True
    ).astype(jnp.float32)
    own_width = summed.shape[1]
    unit_own = tokens.astype(jnp.float32) * inv_rms
    gain_own = lax.dynamic_slice_in_dim(
        gain, lax.axis_index(PLANE) * own_width, own_width, 0
    )
    d_unit = summed * gain_own
    row_sum, gain_part = sums(jnp.sum(unit_own * d_unit, axis=1), jnp.sum(unit_own * summed, axis=0))
    row_mean = row_sum / width
    grad_input = (
        cotangent.astype(jnp.float32) + inv_rms * (d_unit - unit_own * row_mean[:, None])
    ).astype(jnp.bfloat16)
    return grad_input, gain_part


def reduced(tokens, cotangent, gain, w_gate, w_up, w_down):
    full_x = lax.all_gather(tokens, PLANE, axis=1, tiled=True)
    full_dy = lax.all_gather(cotangent, PLANE, axis=1, tiled=True)
    inv_rms, normed = normalise(full_x, gain)
    hidden, d_gate, d_up = hidden_grads(normed, full_dy, w_gate, w_up, w_down)
    grad_down = 0.5 * left_product(hidden, full_dy)
    grad_gate = left_product(d_gate, normed)
    grad_up = left_product(d_up, normed)
    grad_input, gain_part = input_grads(
        tokens, cotangent, gain, inv_rms, hidden_sum(d_gate, d_up, w_gate, w_up),
        lambda rows_part, gain_part: (lax.psum(rows_part, PLANE), gain_part),
    )
    grad_gate, grad_up, grad_down, grad_gain = lax.psum(
        (grad_gate, grad_up, grad_down, gain_part), "rep"
    )
    return (grad_input, grad_gain, grad_gate, grad_up, grad_down)


TILE = 256
BLOCK = 64
MESH = pl.DeviceIdType.MESH
OWN, ACROSS_X, ACROSS_Y, CORNER = range(4)


def step_kernel(
    x_ref, dy_ref, gain_ref, wg_ref, wu_ref, wd_ref,
    grads, act, nrm, dy_tail, gi_ref, gg_ref,
    buf, wts, gain, inv, turned, pair_out, pair_in, own_sum, plane_out, plane_in,
    row_out, row_in, gain_out, gain_in,
    load_sem, send_sem, recv_sem, corner_sem, pair_sem,
    give_sem, take_sem, block_send, block_recv, row_send, row_recv, gain_send, gain_recv,
):
    z, y, t = lax.axis_index("rep"), lax.axis_index("fs"), lax.axis_index("tp")
    rows, cols = x_ref.shape
    hidden, width = wg_ref.shape
    total = 4 * rows
    half = rows // 2
    core = lax.rem(t, 2)
    other = 1 - 2 * core
    x_id = (z, y, lax.rem(t + 2, 4))
    y_id = (z, 1 - y, t)
    corner_id = (z, 1 - y, lax.rem(t + 2, 4))
    pair_id = (z, y, t + other)
    is_end = lax.rem(z + 1, 4) < 2
    is_mid = jnp.logical_not(is_end)
    inner_z = 1 + lax.rem(z, 2)
    inner_id = (inner_z, y, t)
    outer_id = (3 * lax.div(z, 2), y, t)
    inner_slot = 2 - lax.rem(lax.div(z + 1, 2), 2)
    column = (
        y * 4 + t,
        y * 4 + lax.rem(t + 2, 4),
        (1 - y) * 4 + t,
        (1 - y) * 4 + lax.rem(t + 2, 4),
    )
    pair_column = tuple(c + other for c in column)

    def across(col):
        return pl.ds(pl.multiple_of(col * cols, cols), cols)

    def piece(slot, col, p, start=0, size=rows):
        if isinstance(slot, int):
            window = pl.ds(slot * rows + start, size)
        else:
            window = pl.ds(pl.multiple_of(slot * rows + start, 64), size)
        return buf.at[p, window, across(col)]

    sent = []

    def send(make, guard=None):
        if guard is None:
            make().start()
        else:
            pl.when(guard)(lambda: make().start())
        sent.append((make, guard))

    def remote(src, dst, ssem, rsem, target):
        return pltpu.make_async_remote_copy(
            src_ref=src, dst_ref=dst, send_sem=ssem, recv_sem=rsem,
            device_id=target, device_id_type=MESH,
        )

    def arrive(ref, sem):
        pltpu.make_async_remote_copy(
            src_ref=ref, dst_ref=ref, send_sem=send_sem.at[0, 0, 0], recv_sem=sem,
            device_id=pair_id, device_id_type=MESH,
        ).wait_recv()

    def move(slot, q, p, kind, lands, target, start=0, size=rows):
        def make():
            ref = piece(slot, column[q], p, start, size)
            return remote(ref, ref, send_sem.at[kind, slot, p], lands[0].at[lands[1], slot, p], target)

        send(make)

    def to_pair(slot, q, p):
        move(slot, q, p, q, (pair_sem, q), pair_id)

    def to_x(slot, p):
        move(slot, OWN, p, 4, (recv_sem, ACROSS_X), x_id)

    def to_y(slot, p):
        move(slot, OWN, p, 5, (recv_sem, ACROSS_Y), y_id)

    def relay(slot, p):
        move(slot, ACROSS_X, p, 6, (corner_sem, 0), y_id, 0, half)
        move(slot, ACROSS_Y, p, 7, (corner_sem, 1), x_id, half, half)

    def along(slot, q, p, there, kind, target, guard):
        def make():
            return remote(
                piece(slot, column[q], p), piece(there, column[q], p),
                send_sem.at[kind, slot, p], recv_sem.at[q, there, p], target,
            )

        send(make, guard)

    def to_inner(slot, q, p, there, guard=None):
        along(slot, q, p, there, 8 if q == OWN else 9, inner_id, guard)

    def to_outer(slot, q, p, there):
        along(slot, q, p, there, 10 if q == OWN else 11, outer_id, is_mid)

    def landed(slot, q, p):
        arrive(piece(slot, column[q], p), recv_sem.at[q, slot, p])

    def corner_landed(slot, p):
        arrive(piece(slot, column[CORNER], p, 0, half), corner_sem.at[0, slot, p])
        arrive(piece(slot, column[CORNER], p, half, half), corner_sem.at[1, slot, p])

    def pair_landed(slot, p):
        for q in range(4):
            arrive(piece(slot, pair_column[q], p), pair_sem.at[q, slot, p])

    def own_piece(slot, p):
        landed(slot, OWN, p)
        if slot == 1:
            to_outer(1, OWN, p, 2)
        elif slot == 2:
            to_inner(2, OWN, p, 3, is_mid)
        else:
            to_outer(3, OWN, p, 3)
        to_pair(slot, OWN, p)

    def own_across(slot, p):
        to_x(slot, p)
        to_y(slot, p)

    def plane_piece(slot, p):
        landed(slot, ACROSS_X, p)
        landed(slot, ACROSS_Y, p)
        if slot in (0, 3):
            relay(slot, p)
        to_pair(slot, ACROSS_X, p)
        to_pair(slot, ACROSS_Y, p)

    def corner_piece(slot, p):
        if slot in (0, 3):
            corner_landed(slot, p)
        else:
            landed(slot, CORNER, p)
        if slot == 0:
            to_inner(0, CORNER, p, inner_slot)
            to_outer(0, CORNER, p, 1)
        elif slot == 1:
            to_outer(1, CORNER, p, 2)
        to_pair(slot, CORNER, p)

    def guarded(guard, act_on):
        before = len(sent)

        @pl.when(guard)
        def _():
            act_on()

        for i in range(before, len(sent)):
            make, inside = sent[i]
            sent[i] = (make, guard if inside is None else jnp.logical_and(guard, inside))

    loads = [
        pltpu.make_async_copy(ref, piece(0, column[OWN], p), load_sem.at[p])
        for p, ref in enumerate((x_ref, dy_ref))
    ]
    loads.append(pltpu.make_async_copy(gain_ref, gain, load_sem.at[2]))
    for i, ref in enumerate((wg_ref, wu_ref, wd_ref)):
        loads.append(pltpu.make_async_copy(ref, wts.at[i], load_sem.at[3 + i]))
    for load in loads:
        load.start()

    plane_peers = []
    for k in range(1, 8):
        far_y, far_x, far_core = k // 4, (k // 2) % 2, k % 2
        peer_t = lax.rem(t + 2 * far_x, 4)
        if far_core:
            peer_t = peer_t + other
        plane_peers.append((z, lax.rem(y + far_y, 2), peer_t))
    line_peers = [(lax.rem(z + k, 4), y, t) for k in range(1, 4)]
    barrier = pltpu.get_barrier_semaphore()
    for target in plane_peers + line_peers:
        pl.semaphore_signal(barrier, inc=1, device_id=target, device_id_type=MESH)
    pl.semaphore_wait(barrier, len(plane_peers) + len(line_peers))

    def normalise_rows(start, stop):
        gain_row = gain[...]

        def block(i, _):
            window = pl.ds(pl.multiple_of(start + i * BLOCK, BLOCK), BLOCK)
            xf = buf[0, window, :].astype(jnp.float32)
            scale = lax.rsqrt(jnp.sum(xf * xf, axis=1, keepdims=True) / width + EPS)
            nrm[window, :] = (xf * scale * gain_row).astype(jnp.bfloat16)
            if start == 0:
                inv[window, :] = jnp.broadcast_to(scale, (BLOCK, inv.shape[1]))
            return 0

        lax.fori_loop(0, (stop - start) // BLOCK, block, 0)

    def hidden_rows(start, stop, between=(lambda: None, lambda: None)):
        window = slice(start, stop)
        gate = right_product(wts[0], nrm[window, :])
        up = right_product(wts[1], nrm[window, :])
        between[0]()
        d_hidden = 0.5 * right_product(wts[2], buf[1, window, :])
        sig = jax.nn.sigmoid(gate)
        active = gate * sig
        act[0, :, window] = (active * up).astype(jnp.bfloat16)
        act[1, :, window] = (d_hidden * up * sig * (1.0 + gate * (1.0 - sig))).astype(jnp.bfloat16)
        act[2, :, window] = (d_hidden * active).astype(jnp.bfloat16)
        between[1]()

    def weight_grads(start, stop, first, last, fresh):
        window = slice(start, stop)
        step = 2 * TILE

        def tile(j, _):
            span = pl.ds(pl.multiple_of(j * step, step), step)
            for i, right in enumerate((nrm, nrm, None)):
                value = nrm[window, span] if right is not None else buf[1, window, span]
                left = act[(i + 1) % 3, :, window]
                product = jnp.dot(left, value, preferred_element_type=jnp.float32)
                if i == 2:
                    product = 0.5 * product
                if fresh:
                    grads[i, :, span] = product
                else:
                    grads[i, :, span] += product
            return 0

        lax.fori_loop(first * (width // step) // 4, last * (width // step) // 4, tile, 0)

    def feature_product(col):
        span = across(col)
        return jnp.dot(turned[0], wts[0, :, span], preferred_element_type=jnp.float32) + jnp.dot(
            turned[1], wts[1, :, span], preferred_element_type=jnp.float32
        )

    order = (CORNER, ACROSS_X, ACROSS_Y, OWN)
    block_ids = {CORNER: corner_id, ACROSS_X: x_id, ACROSS_Y: y_id}

    def give_pair():
        for i in range(2):
            turned[i] = act[1 + i, :, 0:rows].T
        for k, q in enumerate(order):
            pair_out[k] = feature_product(pair_column[q]).astype(jnp.bfloat16)
            send(lambda k=k: remote(pair_out.at[k], pair_in.at[k], give_sem.at[k], take_sem.at[k], pair_id))

    def give_plane():
        for k, q in enumerate(order):
            product = feature_product(column[q])
            arrive(pair_in.at[k], take_sem.at[k])
            product = product + pair_in[k].astype(jnp.float32)
            if q == OWN:
                own_sum[...] = product
            else:
                plane_out[k] = product.astype(jnp.bfloat16)
                send(lambda k=k, q=q: remote(
                    plane_out.at[k], plane_in.at[k], block_send.at[k], block_recv.at[k], block_ids[q]
                ))

    def own_values():
        unit = buf[0, 0:rows, across(column[OWN])].astype(jnp.float32) * inv[:, 0:1]
        gain_own = gain[0:1, across(column[OWN])]
        return unit, gain_own

    def take_plane():
        for k in range(3):
            arrive(plane_in.at[k], block_recv.at[k])
        summed = own_sum[...]
        for k in range(3):
            summed = summed + plane_in[k].astype(jnp.float32)
        own_sum[...] = summed
        unit, gain_own = own_values()
        product = unit * summed
        gain_out[...] = jnp.broadcast_to(jnp.sum(product, axis=0, keepdims=True), gain_out.shape)
        product = product * gain_own
        lanes = inv.shape[1]
        folded = product[:, 0:lanes]
        for i in range(1, cols // lanes):
            folded = folded + product[:, i * lanes:(i + 1) * lanes]
        row_out[...] = jnp.broadcast_to(jnp.sum(folded.T, axis=0, keepdims=True), row_out.shape)
        for k, target in enumerate(plane_peers):
            send(lambda k=k, target=target: remote(
                row_out, row_in.at[k], row_send.at[k], row_recv.at[k], target
            ))
        for k, target in enumerate(line_peers):
            send(lambda k=k, target=target: remote(
                gain_out, gain_in.at[k], gain_send.at[k], gain_recv.at[k], target
            ))

    def finish_input():
        row = row_out[0:1, :]
        for k in range(7):
            arrive(row_in.at[k], row_recv.at[k])
            row = row + row_in[k, 0:1, :]
        summed_gain = gain_out[...]
        for k in range(3):
            arrive(gain_in.at[k], gain_recv.at[k])
            summed_gain = summed_gain + gain_in[k]
        gg_ref[...] = summed_gain
        lanes = inv.shape[1]
        row_mean = jnp.broadcast_to(row / width, (lanes, rows)).T
        unit, gain_own = own_values()
        d_unit = own_sum[...] * gain_own
        dy_own = buf[1, 0:rows, across(column[OWN])].astype(jnp.float32)
        gi_ref[...] = (dy_own + inv[:, 0:1] * (d_unit - unit * row_mean[:, 0:1])).astype(gi_ref.dtype)

    for p in range(2):
        loads[p].wait()
        to_inner(0, OWN, p, inner_slot)
        to_outer(0, OWN, p, 1)
        to_x(0, p)
        to_y(0, p)
        to_pair(0, OWN, p)
    for p in range(2):
        plane_piece(0, p)
        own_piece(1, p)
        guarded(is_mid, lambda: own_piece(2, p))
    own_across(1, 0)
    own_across(1, 1)

    def middle_across():
        own_across(2, 0)
        own_across(2, 1)

    guarded(is_mid, middle_across)
    corner_piece(0, 0)
    corner_piece(0, 1)
    loads[2].wait()
    pair_landed(0, 0)
    normalise_rows(0, rows)

    def later(p):
        def at_end():
            own_piece(2, p)
            own_across(2, p)

        def at_middle():
            own_piece(3, p)
            own_across(3, p)

        guarded(is_end, at_end)
        guarded(is_mid, at_middle)

    later(0)
    for i in range(3):
        loads[3 + i].wait()
    pair_landed(0, 1)
    hidden_rows(0, rows, (lambda: later(1), lambda: plane_piece(1, 0)))
    give_pair()
    plane_piece(1, 1)
    give_plane()
    corner_piece(1, 0)
    corner_piece(1, 1)
    pair_landed(1, 0)
    pair_landed(1, 1)
    middle = (rows + TILE, rows + 2 * TILE, rows + 3 * TILE)
    normalise_rows(rows, middle[0])
    hidden_rows(rows, middle[0], (lambda: plane_piece(2, 0), lambda: plane_piece(2, 1)))
    split = total // 3

    def end_across(p):
        def act_on():
            own_piece(3, p)
            own_across(3, p)

        guarded(is_end, act_on)

    weight_grads(0, split, 0, 2, True)
    end_across(0)
    weight_grads(0, split, 2, 4, True)
    end_across(1)
    take_plane()
    corner_piece(2, 0)
    corner_piece(2, 1)
    pair_landed(2, 0)
    pair_landed(2, 1)
    normalise_rows(middle[0], middle[1])
    hidden_rows(middle[0], middle[1])
    finish_input()
    normalise_rows(middle[1], middle[2])
    hidden_rows(middle[1], middle[2])
    plane_piece(3, 0)
    weight_grads(split, 2 * split, 0, 2, False)
    plane_piece(3, 1)
    weight_grads(split, 2 * split, 2, 4, False)
    corner_piece(3, 0)
    pair_landed(3, 0)
    normalise_rows(3 * rows, total)

    def rest():
        corner_piece(3, 1)
        pair_landed(3, 1)

    hidden_rows(3 * rows, total, (rest, lambda: None))
    dy_tail[...] = buf[1, 2 * split:, :]
    for make, guard in sent:
        if guard is None:
            make().wait_send()
        else:
            pl.when(guard)(lambda make=make: make().wait_send())


def fused_step(tokens, cotangent, gain, w_gate, w_up, w_down):
    rows, cols = tokens.shape
    hidden, width = w_gate.shape
    total = 4 * rows
    half_type, full_type = jnp.bfloat16, jnp.float32
    hbm = pl.BlockSpec(memory_space=pltpu.HBM)
    vmem = pl.BlockSpec(memory_space=pltpu.VMEM)
    dma = pltpu.SemaphoreType.DMA
    return pl.pallas_call(
        step_kernel,
        out_shape=[
            pltpu.VMEM((3, hidden, width), full_type),
            pltpu.VMEM((3, hidden, total), half_type),
            pltpu.VMEM((total, width), half_type),
            pltpu.VMEM((total // 3, width), half_type),
            pltpu.VMEM((rows, cols), half_type),
            pltpu.VMEM((8, cols), full_type),
        ],
        in_specs=[hbm] * 6,
        out_specs=[vmem] * 6,
        scratch_shapes=[
            pltpu.VMEM((2, total, width), half_type),
            pltpu.VMEM((3, hidden, width), half_type),
            pltpu.VMEM((1, width), full_type),
            pltpu.VMEM((rows, 128), full_type),
            pltpu.VMEM((2, rows, hidden), half_type),
            pltpu.VMEM((4, rows, cols), half_type),
            pltpu.VMEM((4, rows, cols), half_type),
            pltpu.VMEM((rows, cols), full_type),
            pltpu.VMEM((3, rows, cols), half_type),
            pltpu.VMEM((3, rows, cols), half_type),
            pltpu.VMEM((8, rows), full_type),
            pltpu.VMEM((7, 8, rows), full_type),
            pltpu.VMEM((8, cols), full_type),
            pltpu.VMEM((3, 8, cols), full_type),
            dma((6,)), dma((12, 4, 2)), dma((4, 4, 2)), dma((2, 4, 2)), dma((4, 4, 2)),
            dma((4,)), dma((4,)), dma((3,)), dma((3,)), dma((7,)), dma((7,)), dma((3,)), dma((3,)),
        ],
        compiler_params=pltpu.CompilerParams(
            collective_id=0, has_side_effects=True, vmem_limit_bytes=30 * 2**20
        ),
        name="step",
    )(tokens, cotangent, gain.reshape(1, width), w_gate, w_up, w_down)


def last_kernel(grads, act, nrm, dy, gi, gg, gate_ref, up_ref, down_ref, gi_ref, gg_ref, stage, sem):
    width = nrm.shape[1]
    count = dy.shape[0]
    start = nrm.shape[0] - count
    step = 2 * TILE
    outs = (gate_ref, up_ref, down_ref)
    small = [
        pltpu.make_async_copy(gi, gi_ref, sem.at[2, 0]),
        pltpu.make_async_copy(gg, gg_ref, sem.at[2, 1]),
    ]
    for copy in small:
        copy.start()
    waiting = [[], []]
    for j in range(width // step):
        span = slice(j * step, (j + 1) * step)
        slot = j % 2
        for copy in waiting[slot]:
            copy.wait()
        waiting[slot] = []
        for i in range(3):
            left = act[(i + 1) % 3, :, start:]
            value = dy[:, span] if i == 2 else nrm[start:, span]
            product = jnp.dot(left, value, preferred_element_type=jnp.float32)
            if i == 2:
                product = 0.5 * product
            stage[slot, i] = grads[i, :, span] + product
            copy = pltpu.make_async_copy(stage.at[slot, i], outs[i].at[:, span], sem.at[slot, i])
            copy.start()
            waiting[slot].append(copy)
    for copy in waiting[0] + waiting[1] + small:
        copy.wait()


def fused(tokens, cotangent, gain, w_gate, w_up, w_down):
    rows, cols = tokens.shape
    hidden, width = w_gate.shape
    parts = fused_step(tokens, cotangent, gain, w_gate, w_up, w_down)
    full = jax.ShapeDtypeStruct((hidden, width), jnp.float32)
    vmem = pl.BlockSpec(memory_space=pltpu.VMEM)
    grad_gate, grad_up, grad_down, grad_input, grad_gain = pl.pallas_call(
        last_kernel,
        out_shape=[
            full, full, full,
            jax.ShapeDtypeStruct((rows, cols), tokens.dtype),
            jax.ShapeDtypeStruct((8, cols), jnp.float32),
        ],
        in_specs=[vmem] * 6,
        out_specs=[pl.BlockSpec(memory_space=pltpu.HBM)] * 5,
        scratch_shapes=[
            pltpu.VMEM((2, 3, hidden, 2 * TILE), jnp.float32),
            pltpu.SemaphoreType.DMA((3, 3)),
        ],
        compiler_params=pltpu.CompilerParams(vmem_limit_bytes=20 * 2**20),
        name="last",
    )(*parts)
    return grad_input, grad_gain[0], grad_gate, grad_up, grad_down


def fits_fused(tokens, w_gate):
    sizes = tuple(lax.axis_size(name) for name in ("rep", "fs", "tp"))
    rows, cols = tokens.shape
    hidden, width = w_gate.shape
    return (
        sizes == (4, 2, 4)
        and rows == TILE + TILE // 2
        and cols == TILE
        and width == 8 * cols
        and hidden % 16 == 0
        and 24 * hidden * width <= 34 * 2**20
    )


def gathered(tokens, cotangent, gain, w_gate, w_up, w_down):
    rows, cols = tokens.shape
    reps, plane = lax.axis_size("rep"), lax.axis_size(PLANE)
    both = lax.all_gather(jnp.stack([tokens, cotangent]), ("rep",) + PLANE)
    both = both.reshape(reps, plane, 2, rows, cols).transpose(2, 0, 3, 1, 4)
    both = both.reshape(2, reps * rows, plane * cols)
    inv_rms, normed = normalise(both[0], gain)
    dy = both[1]
    hidden, d_gate, d_up = hidden_grads(normed, dy, w_gate, w_up, w_down)
    start = lax.axis_index("rep") * rows
    own = lambda a: lax.dynamic_slice_in_dim(a, start, rows, 0)
    partial_value = hidden_sum(own(d_gate), own(d_up), w_gate, w_up).astype(jnp.bfloat16)
    partial_value, hidden, d_gate, d_up = lax.optimization_barrier(
        (partial_value, hidden, d_gate, d_up)
    )
    grad_input, grad_gain = input_grads(
        tokens, cotangent, gain, own(inv_rms), partial_value, axis_sums
    )
    grad_down = 0.5 * left_product(hidden, dy)
    grad_gate = left_product(d_gate, normed)
    grad_up = left_product(d_up, normed)
    return (grad_input, grad_gain, grad_gate, grad_up, grad_down)


def local(tokens, cotangent, gain, w_gate, w_up, w_down):
    reps = lax.axis_size("rep")
    token_bytes = 2 * 2 * tokens.shape[0] * reps * w_gate.shape[1]
    grad_bytes = 3 * 4 * w_gate.size
    plan = gathered if token_bytes < grad_bytes else reduced
    if fits_fused(tokens, w_gate):
        plan = fused
    return plan(tokens, cotangent, gain, w_gate, w_up, w_down)


def solution(mesh):
    placed = (
        P("rep", PLANE),
        P("rep", PLANE),
        P(),
        P(PLANE, None),
        P(PLANE, None),
        P(PLANE, None),
    )
    return jax.shard_map(
        local,
        mesh=mesh,
        in_specs=placed,
        out_specs=(
            P("rep", PLANE),
            P(PLANE),
            P(PLANE, None),
            P(PLANE, None),
            P(PLANE, None),
        ),
        check_vma=False,
    )
```

```python
import functools

import jax
import jax.numpy as jnp
from jax import lax
from jax.experimental import pallas as pl
from jax.experimental.pallas import tpu as pltpu
from jax.sharding import PartitionSpec as P

EPS = 1e-06
PLANE = ("fs", "tp")


def right_product(left, weight):
    return lax.dot_general(
        left, weight, (((1,), (1,)), ((), ())), preferred_element_type=jnp.float32
    )


def left_product(left, right):
    return lax.dot_general(
        left, right, (((0,), (0,)), ((), ())), preferred_element_type=jnp.float32
    )


def normalise(x, gain):
    xf = x.astype(jnp.float32)
    inv_rms = lax.rsqrt(jnp.mean(xf * xf, axis=1, keepdims=True) + EPS)
    return inv_rms, (xf * inv_rms * gain).astype(jnp.bfloat16)


def hidden_grads(normed, dy, w_gate, w_up, w_down):
    gate = right_product(normed, w_gate)
    up = right_product(normed, w_up)
    sig = jax.nn.sigmoid(gate)
    active = gate * sig
    hidden = (active * up).astype(jnp.bfloat16)
    d_hidden = 0.5 * right_product(dy, w_down)
    d_gate = (d_hidden * up * sig * (1.0 + gate * (1.0 - sig))).astype(jnp.bfloat16)
    d_up = (d_hidden * active).astype(jnp.bfloat16)
    return hidden, d_gate, d_up


def hidden_sum(d_gate, d_up, w_gate, w_up):
    return jnp.dot(d_gate, w_gate, preferred_element_type=jnp.float32) + jnp.dot(
        d_up, w_up, preferred_element_type=jnp.float32
    )


def axis_sums(rows_part, gain_part):
    return lax.psum(rows_part, PLANE), lax.psum(gain_part, "rep")


def input_grads(tokens, cotangent, gain, inv_rms, partial_value, sums):
    width = partial_value.shape[1]
    summed = lax.psum_scatter(
        partial_value, PLANE, scatter_dimension=1, tiled=True
    ).astype(jnp.float32)
    own_width = summed.shape[1]
    unit_own = tokens.astype(jnp.float32) * inv_rms
    gain_own = lax.dynamic_slice_in_dim(
        gain, lax.axis_index(PLANE) * own_width, own_width, 0
    )
    d_unit = summed * gain_own
    row_sum, gain_part = sums(jnp.sum(unit_own * d_unit, axis=1), jnp.sum(unit_own * summed, axis=0))
    row_mean = row_sum / width
    grad_input = (
        cotangent.astype(jnp.float32) + inv_rms * (d_unit - unit_own * row_mean[:, None])
    ).astype(jnp.bfloat16)
    return grad_input, gain_part


def reduced(tokens, cotangent, gain, w_gate, w_up, w_down):
    full_x = lax.all_gather(tokens, PLANE, axis=1, tiled=True)
    full_dy = lax.all_gather(cotangent, PLANE, axis=1, tiled=True)
    inv_rms, normed = normalise(full_x, gain)
    hidden, d_gate, d_up = hidden_grads(normed, full_dy, w_gate, w_up, w_down)
    grad_down = 0.5 * left_product(hidden, full_dy)
    grad_gate = left_product(d_gate, normed)
    grad_up = left_product(d_up, normed)
    grad_input, gain_part = input_grads(
        tokens, cotangent, gain, inv_rms, hidden_sum(d_gate, d_up, w_gate, w_up),
        lambda rows_part, gain_part: (lax.psum(rows_part, PLANE), gain_part),
    )
    grad_gate, grad_up, grad_down, grad_gain = lax.psum(
        (grad_gate, grad_up, grad_down, gain_part), "rep"
    )
    return (grad_input, grad_gain, grad_gate, grad_up, grad_down)


TILE = 256
BLOCK = 64
MESH = pl.DeviceIdType.MESH
OWN, ACROSS_X, ACROSS_Y, CORNER = range(4)


def step_kernel(
    x_ref, dy_ref, gain_ref, wg_ref, wu_ref, wd_ref,
    grad_a, grad_b, grad_c, act_tail, nrm_tail, dy_tail, gi_ref, gg_ref,
    act_main, nrm_main, buf, wts, gain, inv, turned, own_part, pair_out, pair_in, own_sum, plane_out, plane_in,
    row_out, row_in, gain_out, gain_in,
    load_sem, send_sem, recv_sem, corner_sem, pair_sem, late_sem,
    give_sem, take_sem, block_send, block_recv, row_send, row_recv, gain_send, gain_recv,
):
    z, y, t = lax.axis_index("rep"), lax.axis_index("fs"), lax.axis_index("tp")
    rows, cols = x_ref.shape
    hidden, width = wg_ref.shape
    total = 4 * rows
    half = rows // 2
    split = rows + TILE
    core = lax.rem(t, 2)
    other = 1 - 2 * core
    x_id = (z, y, lax.rem(t + 2, 4))
    y_id = (z, 1 - y, t)
    corner_id = (z, 1 - y, lax.rem(t + 2, 4))
    pair_id = (z, y, t + other)
    is_end = lax.rem(z + 1, 4) < 2
    is_mid = jnp.logical_not(is_end)
    inner_z = 1 + lax.rem(z, 2)
    inner_id = (inner_z, y, t)
    outer_id = (3 * lax.div(z, 2), y, t)
    inner_slot = 2 - lax.rem(lax.div(z + 1, 2), 2)
    column = (
        y * 4 + t,
        y * 4 + lax.rem(t + 2, 4),
        (1 - y) * 4 + t,
        (1 - y) * 4 + lax.rem(t + 2, 4),
    )
    pair_column = tuple(c + other for c in column)

    def across(col):
        return pl.ds(pl.multiple_of(col * cols, cols), cols)

    def piece(slot, col, p, start=0, size=rows):
        if isinstance(slot, int):
            window = pl.ds(slot * rows + start, size)
        else:
            window = pl.ds(pl.multiple_of(slot * rows + start, 64), size)
        return buf.at[p, window, across(col)]

    grads = (grad_a, grad_b, grad_c)
    sent = []

    def send(make, guard=None):
        if guard is None:
            make().start()
        else:
            pl.when(guard)(lambda: make().start())
        sent.append((make, () if guard is None else (guard,)))

    def remote(src, dst, ssem, rsem, target):
        return pltpu.make_async_remote_copy(
            src_ref=src, dst_ref=dst, send_sem=ssem, recv_sem=rsem,
            device_id=target, device_id_type=MESH,
        )

    def arrive(ref, sem):
        pltpu.make_async_remote_copy(
            src_ref=ref, dst_ref=ref, send_sem=send_sem.at[0, 0, 0], recv_sem=sem,
            device_id=pair_id, device_id_type=MESH,
        ).wait_recv()

    def move(slot, q, p, kind, lands, target, start=0, size=rows):
        def make():
            ref = piece(slot, column[q], p, start, size)
            return remote(ref, ref, send_sem.at[kind, slot, p], lands[0].at[lands[1], slot, p], target)

        send(make)

    def to_pair(slot, q, p):
        move(slot, q, p, q, (pair_sem, q), pair_id)

    def to_x(slot, p):
        move(slot, OWN, p, 4, (recv_sem, ACROSS_X), x_id)

    def to_y(slot, p):
        move(slot, OWN, p, 5, (recv_sem, ACROSS_Y), y_id)

    def split_across(p, first):
        a, b = (0, half) if first else (half, 0)
        if first:
            move(0, OWN, p, 4, (recv_sem, ACROSS_X), x_id, a, half)
            move(0, OWN, p, 5, (recv_sem, ACROSS_Y), y_id, b, half)
        else:
            move(0, OWN, p, 12, (late_sem, 0), x_id, a, half)
            move(0, OWN, p, 13, (late_sem, 1), y_id, b, half)

    def relay(slot, p):
        move(slot, ACROSS_X, p, 6, (corner_sem, 0), y_id, 0, half)
        move(slot, ACROSS_Y, p, 7, (corner_sem, 1), x_id, half, half)

    def along(slot, q, p, there, kind, target, guard):
        def make():
            return remote(
                piece(slot, column[q], p), piece(there, column[q], p),
                send_sem.at[kind, slot, p], recv_sem.at[q, there, p], target,
            )

        send(make, guard)

    def to_inner(slot, q, p, there, guard=None):
        along(slot, q, p, there, 8 if q == OWN else 9, inner_id, guard)

    def to_outer(slot, q, p, there):
        along(slot, q, p, there, 10 if q == OWN else 11, outer_id, is_mid)

    def landed(slot, q, p):
        arrive(piece(slot, column[q], p), recv_sem.at[q, slot, p])

    def corner_landed(slot, p):
        arrive(piece(slot, column[CORNER], p, 0, half), corner_sem.at[0, slot, p])
        arrive(piece(slot, column[CORNER], p, half, half), corner_sem.at[1, slot, p])

    def pair_landed(slot, p):
        for q in range(4):
            arrive(piece(slot, pair_column[q], p), pair_sem.at[q, slot, p])

    def onward(slot, q, p):
        if slot == 1:
            to_outer(1, q, p, 2)
        elif slot == 2:
            to_inner(2, q, p, 3, is_mid)
        else:
            to_outer(3, q, p, 3)

    def own_piece(slot, p):
        landed(slot, OWN, p)
        onward(slot, OWN, p)
        to_pair(slot, OWN, p)

    def own_across(slot, p):
        to_x(slot, p)
        to_y(slot, p)

    def split_landed(p):
        arrive(piece(0, column[ACROSS_X], p, 0, half), recv_sem.at[ACROSS_X, 0, p])
        arrive(piece(0, column[ACROSS_Y], p, half, half), recv_sem.at[ACROSS_Y, 0, p])
        relay(0, p)

    def split_rest(p):
        arrive(piece(0, column[ACROSS_X], p, half, half), late_sem.at[0, 0, p])
        arrive(piece(0, column[ACROSS_Y], p, 0, half), late_sem.at[1, 0, p])
        to_pair(0, ACROSS_X, p)
        to_pair(0, ACROSS_Y, p)

    def plane_piece(slot, p):
        landed(slot, ACROSS_X, p)
        landed(slot, ACROSS_Y, p)
        if slot == 0:
            relay(0, p)
        elif slot == 1:
            guarded(is_end, lambda: relay(1, p))
        to_pair(slot, ACROSS_X, p)
        to_pair(slot, ACROSS_Y, p)

    def corner_piece(slot, p):
        if slot == 0:
            corner_landed(0, p)
            to_inner(0, CORNER, p, inner_slot)
        elif slot == 1:
            pl.when(is_end)(lambda: corner_landed(1, p))

            def passed_on():
                landed(1, CORNER, p)
                onward(1, CORNER, p)

            guarded(is_mid, passed_on)
        else:
            landed(slot, CORNER, p)
            onward(slot, CORNER, p)
        to_pair(slot, CORNER, p)

    def guarded(guard, act_on):
        before = len(sent)

        @pl.when(guard)
        def _():
            act_on()

        for i in range(before, len(sent)):
            make, inside = sent[i]
            sent[i] = (make, (guard,) + inside)

    loads = [
        pltpu.make_async_copy(ref, piece(0, column[OWN], p), load_sem.at[p])
        for p, ref in enumerate((x_ref, dy_ref))
    ]
    loads.append(pltpu.make_async_copy(gain_ref, gain, load_sem.at[2]))
    for i, ref in enumerate((wg_ref, wu_ref, wd_ref)):
        loads.append(pltpu.make_async_copy(ref, wts.at[i], load_sem.at[3 + i]))
    for load in loads:
        load.start()

    plane_peers = []
    for k in range(1, 8):
        far_y, far_x, far_core = k // 4, (k // 2) % 2, k % 2
        peer_t = lax.rem(t + 2 * far_x, 4)
        if far_core:
            peer_t = peer_t + other
        plane_peers.append((z, lax.rem(y + far_y, 2), peer_t))
    line_peers = [(lax.rem(z + k, 4), y, t) for k in range(1, 4)]
    barrier = pltpu.get_barrier_semaphore()
    for target in plane_peers + line_peers:
        pl.semaphore_signal(barrier, inc=1, device_id=target, device_id_type=MESH)
    pl.semaphore_wait(barrier, len(plane_peers) + len(line_peers))

    def place(start):
        if start < 3 * rows:
            return act_main, nrm_main, start if start < split else start - split
        return act_tail, nrm_tail, start - 3 * rows

    def normalise_rows(start, stop):
        gain_row = gain[...]
        _, nrm, base = place(start)

        def block(i, _):
            window = pl.ds(pl.multiple_of(start + i * BLOCK, BLOCK), BLOCK)
            xf = buf[0, window, :].astype(jnp.float32)
            scale = lax.rsqrt(jnp.sum(xf * xf, axis=1, keepdims=True) / width + EPS)
            nrm[pl.ds(pl.multiple_of(base + i * BLOCK, BLOCK), BLOCK), :] = (
                xf * scale * gain_row
            ).astype(jnp.bfloat16)
            if start == 0:
                inv[window, :] = jnp.broadcast_to(scale, (BLOCK, inv.shape[1]))
            return 0

        lax.fori_loop(0, (stop - start) // BLOCK, block, 0, unroll=2)

    def hidden_rows(start, stop, hooks=()):
        hooks = hooks + (lambda: None,) * (4 - len(hooks))
        last = start == 3 * rows
        act, nrm, base = place(start)
        window = slice(base, base + stop - start)
        gate = right_product(wts[0], nrm[window, :])
        hooks[0]()
        up = right_product(wts[1], nrm[window, :])
        hooks[1]()
        if last:
            dy_tail[...] = buf[1, start:stop, :]
        d_hidden = 0.5 * right_product(wts[2], buf[1, start:stop, :])
        hooks[2]()
        sig = jax.nn.sigmoid(gate)
        active = gate * sig
        act[0, :, window] = (active * up).astype(jnp.bfloat16)
        act[1, :, window] = (d_hidden * up * sig * (1.0 + gate * (1.0 - sig))).astype(jnp.bfloat16)
        act[2, :, window] = (d_hidden * active).astype(jnp.bfloat16)
        hooks[3]()

    def weight_grads(start, stop, first, last, fresh):
        act, nrm, base = place(start)
        window = slice(base, base + stop - start)
        step = 4 * TILE if stop - start == TILE else 2 * TILE

        def tile(j, _):
            span = pl.ds(pl.multiple_of(j * step, step), step)
            for i, right in enumerate((nrm, nrm, None)):
                value = nrm[window, span] if right is not None else buf[1, start:stop, span]
                left = act[(i + 1) % 3, :, window]
                product = jnp.dot(left, value, preferred_element_type=jnp.float32)
                if i == 2:
                    product = 0.5 * product
                if fresh:
                    grads[i][:, span] = product
                else:
                    grads[i][:, span] += product
            return 0

        lax.fori_loop(first * (width // step) // 4, last * (width // step) // 4, tile, 0)

    order = (ACROSS_X, ACROSS_Y, CORNER, OWN)
    block_ids = {CORNER: corner_id, ACROSS_X: x_id, ACROSS_Y: y_id}

    def give_pair():
        for i in range(2):
            turned[i] = act_main[1 + i, :, 0:rows].T
        for k, q in enumerate(order):
            both = pl.ds(pl.multiple_of((column[q] - core) * cols, 2 * cols), 2 * cols)
            product = jnp.dot(turned[0], wts[0, :, both], preferred_element_type=jnp.float32) + jnp.dot(
                turned[1], wts[1, :, both], preferred_element_type=jnp.float32
            )

            def keep(mine, theirs, k=k):
                own_part[k] = mine
                pair_out[k] = theirs.astype(jnp.bfloat16)

            low, high = product[:, :cols], product[:, cols:]
            pl.when(core == 0)(lambda: keep(low, high))
            pl.when(core == 1)(lambda: keep(high, low))
            send(lambda k=k: remote(pair_out.at[k], pair_in.at[k], give_sem.at[k], take_sem.at[k], pair_id))

    def give_plane():
        for k, q in enumerate(order):
            arrive(pair_in.at[k], take_sem.at[k])
            product = own_part[k] + pair_in[k].astype(jnp.float32)
            if q == OWN:
                own_sum[...] = product
            else:
                plane_out[k] = product.astype(jnp.bfloat16)

    def send_plane(k):
        send(lambda: remote(
            plane_out.at[k], plane_in.at[k], block_send.at[k], block_recv.at[k], block_ids[order[k]]
        ))

    def own_values():
        unit = buf[0, 0:rows, across(column[OWN])].astype(jnp.float32) * inv[:, 0:1]
        gain_own = gain[0:1, across(column[OWN])]
        return unit, gain_own

    def take_plane():
        for k in range(3):
            arrive(plane_in.at[k], block_recv.at[k])
        summed = own_sum[...]
        for k in range(3):
            summed = summed + plane_in[k].astype(jnp.float32)
        own_sum[...] = summed
        unit, gain_own = own_values()
        product = unit * summed
        gain_out[...] = jnp.broadcast_to(jnp.sum(product, axis=0, keepdims=True), gain_out.shape)
        product = product * gain_own
        lanes = inv.shape[1]
        folded = product[:, 0:lanes]
        for i in range(1, cols // lanes):
            folded = folded + product[:, i * lanes:(i + 1) * lanes]
        row_out[...] = jnp.broadcast_to(jnp.sum(folded.T, axis=0, keepdims=True), row_out.shape)
        for k, target in enumerate(plane_peers):
            send(lambda k=k, target=target: remote(
                row_out, row_in.at[k], row_send.at[k], row_recv.at[k], target
            ))
        for k, target in enumerate(line_peers):
            send(lambda k=k, target=target: remote(
                gain_out, gain_in.at[k], gain_send.at[k], gain_recv.at[k], target
            ))

    def finish_input():
        row = row_out[0:1, :]
        for k in range(7):
            arrive(row_in.at[k], row_recv.at[k])
            row = row + row_in[k, 0:1, :]
        summed_gain = gain_out[...]
        for k in range(3):
            arrive(gain_in.at[k], gain_recv.at[k])
            summed_gain = summed_gain + gain_in[k]
        gg_ref[...] = summed_gain[0:1, :]
        lanes = inv.shape[1]
        row_mean = jnp.broadcast_to(row / width, (lanes, rows)).T
        unit, gain_own = own_values()
        d_unit = own_sum[...] * gain_own
        dy_own = buf[1, 0:rows, across(column[OWN])].astype(jnp.float32)
        gi_ref[...] = (dy_own + inv[:, 0:1] * (d_unit - unit * row_mean[:, 0:1])).astype(gi_ref.dtype)

    for p in range(2):
        loads[p].wait()
        to_inner(0, OWN, p, inner_slot)
        to_outer(0, OWN, p, 1)
        if p == 0:
            to_x(0, p)
            to_y(0, p)
        else:
            split_across(p, True)
        to_pair(0, OWN, p)
    plane_piece(0, 0)
    split_across(1, False)
    own_piece(1, 0)
    guarded(is_mid, lambda: own_piece(2, 0))
    split_landed(1)
    own_piece(1, 1)
    guarded(is_mid, lambda: own_piece(2, 1))
    corner_piece(0, 0)
    own_across(1, 0)
    own_across(1, 1)

    def middle_across():
        own_across(2, 0)
        own_across(2, 1)

    guarded(is_mid, middle_across)

    def either(at_end, at_mid):
        guarded(is_end, at_end)
        guarded(is_mid, at_mid)

    def all_of(*steps):
        def run():
            for step in steps:
                step()

        return run

    def far_own(p):
        either(lambda: own_piece(2, p), lambda: own_piece(3, p))

    def end_across():
        for p in range(2):
            guarded(is_end, lambda: own_across(2, p))

    def last_own(p):
        either(lambda: own_piece(3, p), lambda: corner_piece(1, p))

    def mid_corner(slot, p):
        guarded(is_mid, lambda: corner_piece(slot, p))

    def end_corner(slot, p):
        guarded(is_end, lambda: corner_piece(slot, p))

    loads[2].wait()
    pair_landed(0, 0)
    normalise_rows(0, rows)
    split_rest(1)
    for i in range(3):
        loads[3 + i].wait()
    hidden_rows(0, rows, (
        all_of(lambda: corner_piece(0, 1), lambda: far_own(0)),
        lambda: pair_landed(0, 1),
        lambda: mid_corner(2, 0),
        all_of(lambda: plane_piece(1, 0), lambda: far_own(1)),
    ))
    give_pair()
    mid_corner(2, 1)
    weight_grads(0, rows, 0, 1, True)
    plane_piece(1, 1)
    end_across()
    last_own(0)
    give_plane()
    end_corner(1, 0)
    weight_grads(0, rows, 1, 3, True)
    last_own(1)
    end_corner(1, 1)
    weight_grads(0, rows, 3, 4, True)
    send_plane(0)
    send_plane(1)
    for p in range(2):
        pair_landed(1, p)
    middle = (rows + TILE, rows + 2 * TILE, rows + 3 * TILE)
    normalise_rows(rows, middle[0])
    hidden_rows(rows, middle[0], (
        lambda: None, lambda: None,
        all_of(lambda: mid_corner(3, 0), lambda: plane_piece(2, 0), lambda: end_corner(2, 0)),
    ))
    send_plane(2)
    weight_grads(rows, middle[0], 0, 4, False)
    plane_piece(2, 1)
    mid_corner(3, 1)
    end_corner(2, 1)
    own_across(3, 0)
    for p in range(2):
        pair_landed(2, p)
    normalise_rows(middle[0], middle[1])
    hidden_rows(middle[0], middle[1], (lambda: None, lambda: end_corner(3, 0)))
    own_across(3, 1)
    normalise_rows(middle[1], middle[2])
    hidden_rows(middle[1], middle[2])
    end_corner(3, 1)
    take_plane()
    weight_grads(split, 3 * rows, 0, 2, False)
    plane_piece(3, 0)
    weight_grads(split, 3 * rows, 2, 4, False)
    finish_input()
    pair_landed(3, 0)
    normalise_rows(3 * rows, total)
    hidden_rows(3 * rows, total, (lambda: plane_piece(3, 1), lambda: pair_landed(3, 1)))
    for make, guards in sent:
        if not guards:
            make().wait_send()
        else:
            pl.when(functools.reduce(jnp.logical_and, guards))(lambda make=make: make().wait_send())


def fused_step(tokens, cotangent, gain, w_gate, w_up, w_down):
    rows, cols = tokens.shape
    hidden, width = w_gate.shape
    total = 4 * rows
    half_type, full_type = jnp.bfloat16, jnp.float32
    hbm = pl.BlockSpec(memory_space=pltpu.HBM)
    vmem = pl.BlockSpec(memory_space=pltpu.VMEM)
    dma = pltpu.SemaphoreType.DMA
    return pl.pallas_call(
        step_kernel,
        out_shape=[
            pltpu.VMEM((hidden, width), full_type),
            pltpu.VMEM((hidden, width), full_type),
            pltpu.VMEM((hidden, width), full_type),
            pltpu.VMEM((3, hidden, rows), half_type),
            pltpu.VMEM((rows, width), half_type),
            pltpu.VMEM((rows, width), half_type),
            pltpu.VMEM((rows, cols), half_type),
            pltpu.VMEM((1, cols), full_type),
        ],
        in_specs=[hbm] * 6,
        out_specs=[vmem] * 8,
        scratch_shapes=[
            pltpu.VMEM((3, hidden, rows + TILE), half_type),
            pltpu.VMEM((rows + TILE, width), half_type),
            pltpu.VMEM((2, total, width), half_type),
            pltpu.VMEM((3, hidden, width), half_type),
            pltpu.VMEM((1, width), full_type),
            pltpu.VMEM((rows, 128), full_type),
            pltpu.VMEM((2, rows, hidden), half_type),
            pltpu.VMEM((4, rows, cols), full_type),
            pltpu.VMEM((4, rows, cols), half_type),
            pltpu.VMEM((4, rows, cols), half_type),
            pltpu.VMEM((rows, cols), full_type),
            pltpu.VMEM((3, rows, cols), half_type),
            pltpu.VMEM((3, rows, cols), half_type),
            pltpu.VMEM((8, rows), full_type),
            pltpu.VMEM((7, 8, rows), full_type),
            pltpu.VMEM((8, cols), full_type),
            pltpu.VMEM((3, 8, cols), full_type),
            dma((6,)), dma((14, 4, 2)), dma((4, 4, 2)), dma((2, 4, 2)), dma((4, 4, 2)), dma((2, 1, 2)),
            dma((4,)), dma((4,)), dma((3,)), dma((3,)), dma((7,)), dma((7,)), dma((3,)), dma((3,)),
        ],
        compiler_params=pltpu.CompilerParams(
            collective_id=0, has_side_effects=True, vmem_limit_bytes=37 * 2**20
        ),
        name="step",
    )(tokens, cotangent, gain.reshape(1, width), w_gate, w_up, w_down)


def last_kernel(grad_a, grad_b, grad_c, act, nrm, dy, gi, gg, gate_ref, up_ref, down_ref, gi_ref, gg_ref, stage, sem):
    width = nrm.shape[1]
    step = 2 * TILE
    grads = (grad_a, grad_b, grad_c)
    outs = (gate_ref, up_ref, down_ref)
    small = [
        pltpu.make_async_copy(gi, gi_ref, sem.at[2, 0]),
        pltpu.make_async_copy(gg, gg_ref, sem.at[2, 1]),
    ]
    for copy in small:
        copy.start()
    waiting = [[], []]
    for j in range(width // step):
        span = slice(j * step, (j + 1) * step)
        slot = j % 2
        for copy in waiting[slot]:
            copy.wait()
        waiting[slot] = []
        for i in range(3):
            left = act[(i + 1) % 3]
            value = dy[:, span] if i == 2 else nrm[:, span]
            product = jnp.dot(left, value, preferred_element_type=jnp.float32)
            if i == 2:
                product = 0.5 * product
            stage[slot, i] = grads[i][:, span] + product
            copy = pltpu.make_async_copy(stage.at[slot, i], outs[i].at[:, span], sem.at[slot, i])
            copy.start()
            waiting[slot].append(copy)
    for copy in waiting[0] + waiting[1] + small:
        copy.wait()


def fused(tokens, cotangent, gain, w_gate, w_up, w_down):
    rows, cols = tokens.shape
    hidden, width = w_gate.shape
    parts = fused_step(tokens, cotangent, gain, w_gate, w_up, w_down)
    full = jax.ShapeDtypeStruct((hidden, width), jnp.float32)
    vmem = pl.BlockSpec(memory_space=pltpu.VMEM)
    grad_gate, grad_up, grad_down, grad_input, grad_gain = pl.pallas_call(
        last_kernel,
        out_shape=[
            full, full, full,
            jax.ShapeDtypeStruct((rows, cols), tokens.dtype),
            jax.ShapeDtypeStruct((1, cols), jnp.float32),
        ],
        in_specs=[vmem] * 8,
        out_specs=[pl.BlockSpec(memory_space=pltpu.HBM)] * 5,
        scratch_shapes=[
            pltpu.VMEM((2, 3, hidden, 2 * TILE), jnp.float32),
            pltpu.SemaphoreType.DMA((3, 3)),
        ],
        compiler_params=pltpu.CompilerParams(vmem_limit_bytes=20 * 2**20),
        name="last",
    )(*parts)
    return grad_input, grad_gain[0], grad_gate, grad_up, grad_down


def fits_fused(tokens, w_gate):
    sizes = tuple(lax.axis_size(name) for name in ("rep", "fs", "tp"))
    rows, cols = tokens.shape
    hidden, width = w_gate.shape
    return (
        sizes == (4, 2, 4)
        and rows == TILE + TILE // 2
        and cols == TILE
        and width == 8 * cols
        and hidden % 16 == 0
        and 24 * hidden * width <= 34 * 2**20
    )


def gathered(tokens, cotangent, gain, w_gate, w_up, w_down):
    rows, cols = tokens.shape
    reps, plane = lax.axis_size("rep"), lax.axis_size(PLANE)
    both = lax.all_gather(jnp.stack([tokens, cotangent]), ("rep",) + PLANE)
    both = both.reshape(reps, plane, 2, rows, cols).transpose(2, 0, 3, 1, 4)
    both = both.reshape(2, reps * rows, plane * cols)
    inv_rms, normed = normalise(both[0], gain)
    dy = both[1]
    hidden, d_gate, d_up = hidden_grads(normed, dy, w_gate, w_up, w_down)
    start = lax.axis_index("rep") * rows
    own = lambda a: lax.dynamic_slice_in_dim(a, start, rows, 0)
    partial_value = hidden_sum(own(d_gate), own(d_up), w_gate, w_up).astype(jnp.bfloat16)
    partial_value, hidden, d_gate, d_up = lax.optimization_barrier(
        (partial_value, hidden, d_gate, d_up)
    )
    grad_input, grad_gain = input_grads(
        tokens, cotangent, gain, own(inv_rms), partial_value, axis_sums
    )
    grad_down = 0.5 * left_product(hidden, dy)
    grad_gate = left_product(d_gate, normed)
    grad_up = left_product(d_up, normed)
    return (grad_input, grad_gain, grad_gate, grad_up, grad_down)


def local(tokens, cotangent, gain, w_gate, w_up, w_down):
    reps = lax.axis_size("rep")
    token_bytes = 2 * 2 * tokens.shape[0] * reps * w_gate.shape[1]
    grad_bytes = 3 * 4 * w_gate.size
    plan = gathered if token_bytes < grad_bytes else reduced
    if fits_fused(tokens, w_gate):
        plan = fused
    return plan(tokens, cotangent, gain, w_gate, w_up, w_down)


def solution(mesh):
    placed = (
        P("rep", PLANE),
        P("rep", PLANE),
        P(),
        P(PLANE, None),
        P(PLANE, None),
        P(PLANE, None),
    )
    return jax.shard_map(
        local,
        mesh=mesh,
        in_specs=placed,
        out_specs=(
            P("rep", PLANE),
            P(PLANE),
            P(PLANE, None),
            P(PLANE, None),
            P(PLANE, None),
        ),
        check_vma=False,
    )
```

```python
import functools

import jax
import jax.numpy as jnp
from jax import lax
from jax.experimental import pallas as pl
from jax.experimental.pallas import tpu as pltpu
from jax.sharding import PartitionSpec as P

EPS = 1e-06
PLANE = ("fs", "tp")


def right_product(left, weight):
    return lax.dot_general(
        left, weight, (((1,), (1,)), ((), ())), preferred_element_type=jnp.float32
    )


def left_product(left, right):
    return lax.dot_general(
        left, right, (((0,), (0,)), ((), ())), preferred_element_type=jnp.float32
    )


def normalise(x, gain):
    xf = x.astype(jnp.float32)
    inv_rms = lax.rsqrt(jnp.mean(xf * xf, axis=1, keepdims=True) + EPS)
    return inv_rms, (xf * inv_rms * gain).astype(jnp.bfloat16)


def hidden_grads(normed, dy, w_gate, w_up, w_down):
    gate = right_product(normed, w_gate)
    up = right_product(normed, w_up)
    sig = jax.nn.sigmoid(gate)
    active = gate * sig
    hidden = (active * up).astype(jnp.bfloat16)
    d_hidden = 0.5 * right_product(dy, w_down)
    d_gate = (d_hidden * up * sig * (1.0 + gate * (1.0 - sig))).astype(jnp.bfloat16)
    d_up = (d_hidden * active).astype(jnp.bfloat16)
    return hidden, d_gate, d_up


def hidden_sum(d_gate, d_up, w_gate, w_up):
    return jnp.dot(d_gate, w_gate, preferred_element_type=jnp.float32) + jnp.dot(
        d_up, w_up, preferred_element_type=jnp.float32
    )


def axis_sums(rows_part, gain_part):
    return lax.psum(rows_part, PLANE), lax.psum(gain_part, "rep")


def input_grads(tokens, cotangent, gain, inv_rms, partial_value, sums):
    width = partial_value.shape[1]
    summed = lax.psum_scatter(
        partial_value, PLANE, scatter_dimension=1, tiled=True
    ).astype(jnp.float32)
    own_width = summed.shape[1]
    unit_own = tokens.astype(jnp.float32) * inv_rms
    gain_own = lax.dynamic_slice_in_dim(
        gain, lax.axis_index(PLANE) * own_width, own_width, 0
    )
    d_unit = summed * gain_own
    row_sum, gain_part = sums(jnp.sum(unit_own * d_unit, axis=1), jnp.sum(unit_own * summed, axis=0))
    row_mean = row_sum / width
    grad_input = (
        cotangent.astype(jnp.float32) + inv_rms * (d_unit - unit_own * row_mean[:, None])
    ).astype(jnp.bfloat16)
    return grad_input, gain_part


def reduced(tokens, cotangent, gain, w_gate, w_up, w_down):
    full_x = lax.all_gather(tokens, PLANE, axis=1, tiled=True)
    full_dy = lax.all_gather(cotangent, PLANE, axis=1, tiled=True)
    inv_rms, normed = normalise(full_x, gain)
    hidden, d_gate, d_up = hidden_grads(normed, full_dy, w_gate, w_up, w_down)
    grad_down = 0.5 * left_product(hidden, full_dy)
    grad_gate = left_product(d_gate, normed)
    grad_up = left_product(d_up, normed)
    grad_input, gain_part = input_grads(
        tokens, cotangent, gain, inv_rms, hidden_sum(d_gate, d_up, w_gate, w_up),
        lambda rows_part, gain_part: (lax.psum(rows_part, PLANE), gain_part),
    )
    grad_gate, grad_up, grad_down, grad_gain = lax.psum(
        (grad_gate, grad_up, grad_down, gain_part), "rep"
    )
    return (grad_input, grad_gain, grad_gate, grad_up, grad_down)


TILE = 256
BLOCK = 64
MESH = pl.DeviceIdType.MESH
OWN, ACROSS_X, ACROSS_Y, CORNER = range(4)


def step_kernel(
    x_ref, dy_ref, gain_ref, wg_ref, wu_ref, wd_ref,
    grad_a, grad_b, grad_c, act_tail, nrm_tail, dy_tail, gi_ref, gg_ref,
    act_main, nrm_main, buf, wts, gain, inv, turned, own_part, pair_out, pair_in, own_sum, plane_out, plane_in,
    row_out, row_in, gain_out, gain_in,
    load_sem, send_sem, recv_sem, line_own, line_corner, corner_sem, pair_sem, late_sem,
    give_sem, take_sem, block_send, block_recv, row_send, row_recv, gain_send, gain_recv,
):
    z, y, t = lax.axis_index("rep"), lax.axis_index("fs"), lax.axis_index("tp")
    rows, cols = x_ref.shape
    hidden, width = wg_ref.shape
    total = 4 * rows
    half = rows // 2
    split = rows + TILE
    core = lax.rem(t, 2)
    other = 1 - 2 * core
    x_id = (z, y, lax.rem(t + 2, 4))
    y_id = (z, 1 - y, t)
    corner_id = (z, 1 - y, lax.rem(t + 2, 4))
    pair_id = (z, y, t + other)
    is_end = lax.rem(z + 1, 4) < 2
    is_mid = jnp.logical_not(is_end)
    inner_z = 1 + lax.rem(z, 2)
    inner_id = (inner_z, y, t)
    outer_id = (3 * lax.div(z, 2), y, t)
    inner_slot = 2 - lax.rem(lax.div(z + 1, 2), 2)
    column = (
        y * 4 + t,
        y * 4 + lax.rem(t + 2, 4),
        (1 - y) * 4 + t,
        (1 - y) * 4 + lax.rem(t + 2, 4),
    )
    pair_column = tuple(c + other for c in column)

    def across(col):
        return pl.ds(pl.multiple_of(col * cols, cols), cols)

    def piece(slot, col, p, start=0, size=rows):
        if isinstance(slot, int):
            window = pl.ds(slot * rows + start, size)
        else:
            window = pl.ds(pl.multiple_of(slot * rows + start, 64), size)
        return buf.at[p, window, across(col)]

    grads = (grad_a, grad_b, grad_c)
    sent = []
    numbers = {}

    def number(*key):
        return numbers.setdefault(key, len(numbers))


    def send(make, guard=None):
        if guard is None:
            make().start()
        else:
            pl.when(guard)(lambda: make().start())
        sent.append((make, () if guard is None else (guard,)))

    def remote(src, dst, ssem, rsem, target):
        return pltpu.make_async_remote_copy(
            src_ref=src, dst_ref=dst, send_sem=ssem, recv_sem=rsem,
            device_id=target, device_id_type=MESH,
        )

    def arrive(ref, sem):
        pltpu.make_async_remote_copy(
            src_ref=ref, dst_ref=ref, send_sem=send_sem.at[0], recv_sem=sem,
            device_id=pair_id, device_id_type=MESH,
        ).wait_recv()

    def move(slot, q, p, kind, lands, target, start=0, size=rows):
        own_number = number(kind, slot, p)

        def make():
            ref = piece(slot, column[q], p, start, size)
            return remote(ref, ref, send_sem.at[own_number], lands[0].at[lands[1], slot, p], target)

        send(make)

    def to_pair(slot, q, p):
        move(slot, q, p, q, (pair_sem, q), pair_id)

    def to_x(slot, p):
        move(slot, OWN, p, 4, (recv_sem, 0), x_id)

    def to_y(slot, p):
        move(slot, OWN, p, 5, (recv_sem, 1), y_id)

    def split_across(p, first):
        a, b = (0, half) if first else (half, 0)
        if first:
            move(0, OWN, p, 4, (recv_sem, 0), x_id, a, half)
            move(0, OWN, p, 5, (recv_sem, 1), y_id, b, half)
        else:
            move(0, OWN, p, 12, (late_sem, 0), x_id, a, half)
            move(0, OWN, p, 13, (late_sem, 1), y_id, b, half)

    def relay(slot, p):
        move(slot, ACROSS_X, p, 6, (corner_sem, 0), y_id, 0, half)
        move(slot, ACROSS_Y, p, 7, (corner_sem, 1), x_id, half, half)

    def along(slot, q, p, there, kind, target, guard):
        own_number = number(kind, slot, p)
        line = line_own if q == OWN else line_corner

        def make():
            return remote(
                piece(slot, column[q], p), piece(there, column[q], p),
                send_sem.at[own_number], line.at[there - 1, p], target,
            )

        send(make, guard)

    def to_inner(slot, q, p, there, guard=None):
        along(slot, q, p, there, 8 if q == OWN else 9, inner_id, guard)

    def to_outer(slot, q, p, there):
        along(slot, q, p, there, 10 if q == OWN else 11, outer_id, is_mid)

    def landed(slot, q, p):
        if q in (ACROSS_X, ACROSS_Y):
            sem = recv_sem.at[q - 1, slot, p]
        else:
            sem = (line_own if q == OWN else line_corner).at[slot - 1, p]
        arrive(piece(slot, column[q], p), sem)

    def corner_landed(slot, p):
        arrive(piece(slot, column[CORNER], p, 0, half), corner_sem.at[0, slot, p])
        arrive(piece(slot, column[CORNER], p, half, half), corner_sem.at[1, slot, p])

    def pair_landed(slot, p):
        for q in range(4):
            arrive(piece(slot, pair_column[q], p), pair_sem.at[q, slot, p])

    def onward(slot, q, p):
        if slot == 1:
            to_outer(1, q, p, 2)
        elif slot == 2:
            to_inner(2, q, p, 3, is_mid)
        else:
            to_outer(3, q, p, 3)

    def own_piece(slot, p):
        landed(slot, OWN, p)
        onward(slot, OWN, p)
        to_pair(slot, OWN, p)

    def own_across(slot, p):
        to_x(slot, p)
        to_y(slot, p)

    def split_landed(p):
        arrive(piece(0, column[ACROSS_X], p, 0, half), recv_sem.at[0, 0, p])
        arrive(piece(0, column[ACROSS_Y], p, half, half), recv_sem.at[1, 0, p])
        relay(0, p)

    def split_rest(p):
        arrive(piece(0, column[ACROSS_X], p, half, half), late_sem.at[0, 0, p])
        arrive(piece(0, column[ACROSS_Y], p, 0, half), late_sem.at[1, 0, p])
        to_pair(0, ACROSS_X, p)
        to_pair(0, ACROSS_Y, p)

    def plane_piece(slot, p):
        landed(slot, ACROSS_X, p)
        landed(slot, ACROSS_Y, p)
        if slot == 0:
            relay(0, p)
        elif slot == 1:
            guarded(is_end, lambda: relay(1, p))
        to_pair(slot, ACROSS_X, p)
        to_pair(slot, ACROSS_Y, p)

    def corner_piece(slot, p):
        if slot == 0:
            corner_landed(0, p)
            to_inner(0, CORNER, p, inner_slot)
        elif slot == 1:
            pl.when(is_end)(lambda: corner_landed(1, p))

            def passed_on():
                landed(1, CORNER, p)
                onward(1, CORNER, p)

            guarded(is_mid, passed_on)
        else:
            landed(slot, CORNER, p)
            onward(slot, CORNER, p)
        to_pair(slot, CORNER, p)

    def guarded(guard, act_on):
        before = len(sent)

        @pl.when(guard)
        def _():
            act_on()

        for i in range(before, len(sent)):
            make, inside = sent[i]
            sent[i] = (make, (guard,) + inside)

    loads = [
        pltpu.make_async_copy(ref, piece(0, column[OWN], p), load_sem.at[p])
        for p, ref in enumerate((x_ref, dy_ref))
    ]
    loads.append(pltpu.make_async_copy(gain_ref, gain, load_sem.at[2]))
    for i, ref in enumerate((wg_ref, wu_ref, wd_ref)):
        loads.append(pltpu.make_async_copy(ref, wts.at[i], load_sem.at[3 + i]))
    for load in loads:
        load.start()

    plane_peers = []
    for k in range(1, 8):
        far_y, far_x, far_core = k // 4, (k // 2) % 2, k % 2
        peer_t = lax.rem(t + 2 * far_x, 4)
        if far_core:
            peer_t = peer_t + other
        plane_peers.append((z, lax.rem(y + far_y, 2), peer_t))
    line_peers = [(lax.rem(z + k, 4), y, t) for k in range(1, 4)]
    barrier = pltpu.get_barrier_semaphore()
    for target in plane_peers + line_peers:
        pl.semaphore_signal(barrier, inc=1, device_id=target, device_id_type=MESH)
    pl.semaphore_wait(barrier, len(plane_peers) + len(line_peers))

    def place(start):
        if start < 3 * rows:
            return act_main, nrm_main, start if start < split else start - split
        return act_tail, nrm_tail, start - 3 * rows

    def normalise_rows(start, stop):
        gain_row = gain[...]
        _, nrm, base = place(start)

        def block(i, _):
            window = pl.ds(pl.multiple_of(start + i * BLOCK, BLOCK), BLOCK)
            xf = buf[0, window, :].astype(jnp.float32)
            scale = lax.rsqrt(jnp.sum(xf * xf, axis=1, keepdims=True) / width + EPS)
            nrm[pl.ds(pl.multiple_of(base + i * BLOCK, BLOCK), BLOCK), :] = (
                xf * scale * gain_row
            ).astype(jnp.bfloat16)
            if start == 0:
                inv[window, :] = jnp.broadcast_to(scale, (BLOCK, inv.shape[1]))
            return 0

        lax.fori_loop(0, (stop - start) // BLOCK, block, 0, unroll=2)

    def hidden_rows(start, stop, hooks=()):
        hooks = hooks + (lambda: None,) * (4 - len(hooks))
        last = start == 3 * rows
        act, nrm, base = place(start)
        window = slice(base, base + stop - start)
        gate = right_product(wts[0], nrm[window, :])
        hooks[0]()
        up = right_product(wts[1], nrm[window, :])
        hooks[1]()
        if last:
            dy_tail[...] = buf[1, start:stop, :]
        d_hidden = 0.5 * right_product(wts[2], buf[1, start:stop, :])
        hooks[2]()
        sig = jax.nn.sigmoid(gate)
        active = gate * sig
        act[0, :, window] = (active * up).astype(jnp.bfloat16)
        act[1, :, window] = (d_hidden * up * sig * (1.0 + gate * (1.0 - sig))).astype(jnp.bfloat16)
        act[2, :, window] = (d_hidden * active).astype(jnp.bfloat16)
        hooks[3]()

    def weight_grads(start, stop, first, last, fresh):
        act, nrm, base = place(start)
        window = slice(base, base + stop - start)
        step = 4 * TILE if stop - start == TILE else 2 * TILE

        def tile(j, _):
            span = pl.ds(pl.multiple_of(j * step, step), step)
            for i, right in enumerate((nrm, nrm, None)):
                value = nrm[window, span] if right is not None else buf[1, start:stop, span]
                left = act[(i + 1) % 3, :, window]
                product = jnp.dot(left, value, preferred_element_type=jnp.float32)
                if i == 2:
                    product = 0.5 * product
                if fresh:
                    grads[i][:, span] = product
                else:
                    grads[i][:, span] += product
            return 0

        lax.fori_loop(first * (width // step) // 4, last * (width // step) // 4, tile, 0)

    order = (ACROSS_X, ACROSS_Y, CORNER, OWN)
    block_ids = {CORNER: corner_id, ACROSS_X: x_id, ACROSS_Y: y_id}

    def give_pair():
        for i in range(2):
            turned[i] = act_main[1 + i, :, 0:rows].T
        for k, q in enumerate(order):
            both = pl.ds(pl.multiple_of((column[q] - core) * cols, 2 * cols), 2 * cols)
            product = jnp.dot(turned[0], wts[0, :, both], preferred_element_type=jnp.float32) + jnp.dot(
                turned[1], wts[1, :, both], preferred_element_type=jnp.float32
            )

            def keep(mine, theirs, k=k):
                own_part[k] = mine
                pair_out[k] = theirs.astype(jnp.bfloat16)

            low, high = product[:, :cols], product[:, cols:]
            pl.when(core == 0)(lambda: keep(low, high))
            pl.when(core == 1)(lambda: keep(high, low))
            send(lambda k=k: remote(pair_out.at[k], pair_in.at[k], give_sem.at[k], take_sem.at[k], pair_id))

    def give_plane():
        for k, q in enumerate(order):
            arrive(pair_in.at[k], take_sem.at[k])
            product = own_part[k] + pair_in[k].astype(jnp.float32)
            if q == OWN:
                own_sum[...] = product
            else:
                plane_out[k] = product.astype(jnp.bfloat16)

    def send_plane(k):
        send(lambda: remote(
            plane_out.at[k], plane_in.at[k], block_send.at[k], block_recv.at[k], block_ids[order[k]]
        ))

    def own_values():
        unit = buf[0, 0:rows, across(column[OWN])].astype(jnp.float32) * inv[:, 0:1]
        gain_own = gain[0:1, across(column[OWN])]
        return unit, gain_own

    def take_plane():
        for k in range(3):
            arrive(plane_in.at[k], block_recv.at[k])
        summed = own_sum[...]
        for k in range(3):
            summed = summed + plane_in[k].astype(jnp.float32)
        own_sum[...] = summed
        unit, gain_own = own_values()
        product = unit * summed
        gain_out[...] = jnp.broadcast_to(jnp.sum(product, axis=0, keepdims=True), gain_out.shape)
        product = product * gain_own
        lanes = inv.shape[1]
        folded = product[:, 0:lanes]
        for i in range(1, cols // lanes):
            folded = folded + product[:, i * lanes:(i + 1) * lanes]
        row_out[...] = jnp.broadcast_to(jnp.sum(folded.T, axis=0, keepdims=True), row_out.shape)
        for k, target in enumerate(plane_peers):
            send(lambda k=k, target=target: remote(
                row_out, row_in.at[k], row_send.at[k], row_recv.at[k], target
            ))
        for k, target in enumerate(line_peers):
            send(lambda k=k, target=target: remote(
                gain_out, gain_in.at[k], gain_send.at[k], gain_recv.at[k], target
            ))

    def finish_input():
        row = row_out[0:1, :]
        for k in range(7):
            arrive(row_in.at[k], row_recv.at[k])
            row = row + row_in[k, 0:1, :]
        summed_gain = gain_out[...]
        for k in range(3):
            arrive(gain_in.at[k], gain_recv.at[k])
            summed_gain = summed_gain + gain_in[k]
        gg_ref[...] = summed_gain[0:1, :]
        lanes = inv.shape[1]
        row_mean = jnp.broadcast_to(row / width, (lanes, rows)).T
        unit, gain_own = own_values()
        d_unit = own_sum[...] * gain_own
        dy_own = buf[1, 0:rows, across(column[OWN])].astype(jnp.float32)
        gi_ref[...] = (dy_own + inv[:, 0:1] * (d_unit - unit * row_mean[:, 0:1])).astype(gi_ref.dtype)

    for p in range(2):
        loads[p].wait()
        to_inner(0, OWN, p, inner_slot)
        to_outer(0, OWN, p, 1)
        if p == 0:
            to_x(0, p)
            to_y(0, p)
        else:
            split_across(p, True)
        to_pair(0, OWN, p)
    plane_piece(0, 0)
    split_across(1, False)
    own_piece(1, 0)
    guarded(is_mid, lambda: own_piece(2, 0))
    split_landed(1)
    own_piece(1, 1)
    guarded(is_mid, lambda: own_piece(2, 1))
    corner_piece(0, 0)
    own_across(1, 0)
    own_across(1, 1)

    def middle_across():
        own_across(2, 0)
        own_across(2, 1)

    guarded(is_mid, middle_across)

    def either(at_end, at_mid):
        guarded(is_end, at_end)
        guarded(is_mid, at_mid)

    def all_of(*steps):
        def run():
            for step in steps:
                step()

        return run

    def far_own(p):
        either(lambda: own_piece(2, p), lambda: own_piece(3, p))

    def end_across():
        for p in range(2):
            guarded(is_end, lambda: own_across(2, p))

    def last_own(p):
        either(lambda: own_piece(3, p), lambda: corner_piece(1, p))

    def mid_corner(slot, p):
        guarded(is_mid, lambda: corner_piece(slot, p))

    def end_corner(slot, p):
        guarded(is_end, lambda: corner_piece(slot, p))

    loads[2].wait()
    pair_landed(0, 0)
    normalise_rows(0, rows)
    split_rest(1)
    for i in range(3):
        loads[3 + i].wait()
    hidden_rows(0, rows, (
        all_of(lambda: corner_piece(0, 1), lambda: far_own(0)),
        lambda: pair_landed(0, 1),
        lambda: mid_corner(2, 0),
        all_of(lambda: plane_piece(1, 0), lambda: far_own(1)),
    ))
    give_pair()
    mid_corner(2, 1)
    plane_piece(1, 1)
    end_across()
    weight_grads(0, rows, 0, 1, True)
    last_own(0)
    give_plane()
    end_corner(1, 0)
    weight_grads(0, rows, 1, 3, True)
    last_own(1)
    end_corner(1, 1)
    weight_grads(0, rows, 3, 4, True)
    send_plane(0)
    send_plane(1)
    pair_landed(1, 0)
    middle = (rows + TILE, rows + 2 * TILE, rows + 3 * TILE)
    normalise_rows(rows, middle[0])
    hidden_rows(rows, middle[0], (
        lambda: None, lambda: pair_landed(1, 1),
        all_of(lambda: mid_corner(3, 0), lambda: plane_piece(2, 0), lambda: end_corner(2, 0)),
    ))
    send_plane(2)
    weight_grads(rows, middle[0], 0, 2, False)
    own_across(3, 0)
    weight_grads(rows, middle[0], 2, 4, False)
    pair_landed(2, 0)
    normalise_rows(middle[0], middle[1])
    plane_piece(2, 1)
    mid_corner(3, 1)
    end_corner(2, 1)
    hidden_rows(middle[0], middle[1], (lambda: None, all_of(lambda: end_corner(3, 0), lambda: pair_landed(2, 1))))
    own_across(3, 1)
    normalise_rows(middle[1], middle[2])
    hidden_rows(middle[1], middle[2])
    end_corner(3, 1)
    take_plane()
    weight_grads(split, 3 * rows, 0, 3, False)
    plane_piece(3, 0)
    weight_grads(split, 3 * rows, 3, 4, False)
    pair_landed(3, 0)
    normalise_rows(3 * rows, total)
    hidden_rows(3 * rows, total, (
        lambda: plane_piece(3, 1), all_of(finish_input, lambda: pair_landed(3, 1)),
    ))
    for make, guards in sent:
        if not guards:
            make().wait_send()
        else:
            pl.when(functools.reduce(jnp.logical_and, guards))(lambda make=make: make().wait_send())


def fused_step(tokens, cotangent, gain, w_gate, w_up, w_down):
    rows, cols = tokens.shape
    hidden, width = w_gate.shape
    total = 4 * rows
    half_type, full_type = jnp.bfloat16, jnp.float32
    hbm = pl.BlockSpec(memory_space=pltpu.HBM)
    vmem = pl.BlockSpec(memory_space=pltpu.VMEM)
    dma = pltpu.SemaphoreType.DMA
    return pl.pallas_call(
        step_kernel,
        out_shape=[
            pltpu.VMEM((hidden, width), full_type),
            pltpu.VMEM((hidden, width), full_type),
            pltpu.VMEM((hidden, width), full_type),
            pltpu.VMEM((3, hidden, rows), half_type),
            pltpu.VMEM((rows, width), half_type),
            pltpu.VMEM((rows, width), half_type),
            pltpu.VMEM((rows, cols), half_type),
            pltpu.VMEM((1, cols), full_type),
        ],
        in_specs=[hbm] * 6,
        out_specs=[vmem] * 8,
        scratch_shapes=[
            pltpu.VMEM((3, hidden, rows + TILE), half_type),
            pltpu.VMEM((rows + TILE, width), half_type),
            pltpu.VMEM((2, total, width), half_type),
            pltpu.VMEM((3, hidden, width), half_type),
            pltpu.VMEM((1, width), full_type),
            pltpu.VMEM((rows, 128), full_type),
            pltpu.VMEM((2, rows, hidden), half_type),
            pltpu.VMEM((4, rows, cols), full_type),
            pltpu.VMEM((4, rows, cols), half_type),
            pltpu.VMEM((4, rows, cols), half_type),
            pltpu.VMEM((rows, cols), full_type),
            pltpu.VMEM((3, rows, cols), half_type),
            pltpu.VMEM((3, rows, cols), half_type),
            pltpu.VMEM((8, rows), full_type),
            pltpu.VMEM((7, 8, rows), full_type),
            pltpu.VMEM((8, cols), full_type),
            pltpu.VMEM((3, 8, cols), full_type),
            dma((6,)), dma((76,)), dma((2, 4, 2)), dma((3, 2)), dma((3, 2)),
            dma((2, 2, 2)), dma((4, 4, 2)), dma((2, 1, 2)),
            dma((4,)), dma((4,)), dma((3,)), dma((3,)), dma((7,)), dma((7,)), dma((3,)), dma((3,)),
        ],
        compiler_params=pltpu.CompilerParams(
            collective_id=0, has_side_effects=True, vmem_limit_bytes=37 * 2**20
        ),
        name="step",
    )(tokens, cotangent, gain.reshape(1, width), w_gate, w_up, w_down)


def last_kernel(grad_a, grad_b, grad_c, act, nrm, dy, gi, gg, gate_ref, up_ref, down_ref, gi_ref, gg_ref, stage, sem):
    width = nrm.shape[1]
    step = 2 * TILE
    grads = (grad_a, grad_b, grad_c)
    outs = (gate_ref, up_ref, down_ref)
    small = [
        pltpu.make_async_copy(gi, gi_ref, sem.at[2, 0]),
        pltpu.make_async_copy(gg, gg_ref, sem.at[2, 1]),
    ]
    for copy in small:
        copy.start()
    waiting = [[], []]
    for j in range(width // step):
        span = slice(j * step, (j + 1) * step)
        slot = j % 2
        for copy in waiting[slot]:
            copy.wait()
        waiting[slot] = []
        for i in range(3):
            left = act[(i + 1) % 3]
            value = dy[:, span] if i == 2 else nrm[:, span]
            product = jnp.dot(left, value, preferred_element_type=jnp.float32)
            if i == 2:
                product = 0.5 * product
            stage[slot, i] = grads[i][:, span] + product
            copy = pltpu.make_async_copy(stage.at[slot, i], outs[i].at[:, span], sem.at[slot, i])
            copy.start()
            waiting[slot].append(copy)
    for copy in waiting[0] + waiting[1] + small:
        copy.wait()


def fused(tokens, cotangent, gain, w_gate, w_up, w_down):
    rows, cols = tokens.shape
    hidden, width = w_gate.shape
    parts = fused_step(tokens, cotangent, gain, w_gate, w_up, w_down)
    full = jax.ShapeDtypeStruct((hidden, width), jnp.float32)
    vmem = pl.BlockSpec(memory_space=pltpu.VMEM)
    grad_gate, grad_up, grad_down, grad_input, grad_gain = pl.pallas_call(
        last_kernel,
        out_shape=[
            full, full, full,
            jax.ShapeDtypeStruct((rows, cols), tokens.dtype),
            jax.ShapeDtypeStruct((1, cols), jnp.float32),
        ],
        in_specs=[vmem] * 8,
        out_specs=[pl.BlockSpec(memory_space=pltpu.HBM)] * 5,
        scratch_shapes=[
            pltpu.VMEM((2, 3, hidden, 2 * TILE), jnp.float32),
            pltpu.SemaphoreType.DMA((3, 3)),
        ],
        compiler_params=pltpu.CompilerParams(vmem_limit_bytes=20 * 2**20),
        name="last",
    )(*parts)
    return grad_input, grad_gain[0], grad_gate, grad_up, grad_down


def fits_fused(tokens, w_gate):
    sizes = tuple(lax.axis_size(name) for name in ("rep", "fs", "tp"))
    rows, cols = tokens.shape
    hidden, width = w_gate.shape
    return (
        sizes == (4, 2, 4)
        and rows == TILE + TILE // 2
        and cols == TILE
        and width == 8 * cols
        and hidden % 16 == 0
        and 24 * hidden * width <= 34 * 2**20
    )


def gathered(tokens, cotangent, gain, w_gate, w_up, w_down):
    rows, cols = tokens.shape
    reps, plane = lax.axis_size("rep"), lax.axis_size(PLANE)
    both = lax.all_gather(jnp.stack([tokens, cotangent]), ("rep",) + PLANE)
    both = both.reshape(reps, plane, 2, rows, cols).transpose(2, 0, 3, 1, 4)
    both = both.reshape(2, reps * rows, plane * cols)
    inv_rms, normed = normalise(both[0], gain)
    dy = both[1]
    hidden, d_gate, d_up = hidden_grads(normed, dy, w_gate, w_up, w_down)
    start = lax.axis_index("rep") * rows
    own = lambda a: lax.dynamic_slice_in_dim(a, start, rows, 0)
    partial_value = hidden_sum(own(d_gate), own(d_up), w_gate, w_up).astype(jnp.bfloat16)
    partial_value, hidden, d_gate, d_up = lax.optimization_barrier(
        (partial_value, hidden, d_gate, d_up)
    )
    grad_input, grad_gain = input_grads(
        tokens, cotangent, gain, own(inv_rms), partial_value, axis_sums
    )
    grad_down = 0.5 * left_product(hidden, dy)
    grad_gate = left_product(d_gate, normed)
    grad_up = left_product(d_up, normed)
    return (grad_input, grad_gain, grad_gate, grad_up, grad_down)


def local(tokens, cotangent, gain, w_gate, w_up, w_down):
    reps = lax.axis_size("rep")
    token_bytes = 2 * 2 * tokens.shape[0] * reps * w_gate.shape[1]
    grad_bytes = 3 * 4 * w_gate.size
    plan = gathered if token_bytes < grad_bytes else reduced
    if fits_fused(tokens, w_gate):
        plan = fused
    return plan(tokens, cotangent, gain, w_gate, w_up, w_down)


def solution(mesh):
    placed = (
        P("rep", PLANE),
        P("rep", PLANE),
        P(),
        P(PLANE, None),
        P(PLANE, None),
        P(PLANE, None),
    )
    return jax.shard_map(
        local,
        mesh=mesh,
        in_specs=placed,
        out_specs=(
            P("rep", PLANE),
            P(PLANE),
            P(PLANE, None),
            P(PLANE, None),
            P(PLANE, None),
        ),
        check_vma=False,
    )
```

```python
import functools

import jax
import jax.numpy as jnp
from jax import lax
from jax.experimental import pallas as pl
from jax.experimental.pallas import tpu as pltpu
from jax.sharding import PartitionSpec as P

EPS = 1e-06
PLANE = ("fs", "tp")


def right_product(left, weight):
    return lax.dot_general(
        left, weight, (((1,), (1,)), ((), ())), preferred_element_type=jnp.float32
    )


def left_product(left, right):
    return lax.dot_general(
        left, right, (((0,), (0,)), ((), ())), preferred_element_type=jnp.float32
    )


def normalise(x, gain):
    xf = x.astype(jnp.float32)
    inv_rms = lax.rsqrt(jnp.mean(xf * xf, axis=1, keepdims=True) + EPS)
    return inv_rms, (xf * inv_rms * gain).astype(jnp.bfloat16)


def hidden_grads(normed, dy, w_gate, w_up, w_down):
    gate = right_product(normed, w_gate)
    up = right_product(normed, w_up)
    sig = jax.nn.sigmoid(gate)
    active = gate * sig
    hidden = (active * up).astype(jnp.bfloat16)
    d_hidden = 0.5 * right_product(dy, w_down)
    d_gate = (d_hidden * up * sig * (1.0 + gate * (1.0 - sig))).astype(jnp.bfloat16)
    d_up = (d_hidden * active).astype(jnp.bfloat16)
    return hidden, d_gate, d_up


def hidden_sum(d_gate, d_up, w_gate, w_up):
    return jnp.dot(d_gate, w_gate, preferred_element_type=jnp.float32) + jnp.dot(
        d_up, w_up, preferred_element_type=jnp.float32
    )


def axis_sums(rows_part, gain_part):
    return lax.psum(rows_part, PLANE), lax.psum(gain_part, "rep")


def input_grads(tokens, cotangent, gain, inv_rms, partial_value, sums):
    width = partial_value.shape[1]
    summed = lax.psum_scatter(
        partial_value, PLANE, scatter_dimension=1, tiled=True
    ).astype(jnp.float32)
    own_width = summed.shape[1]
    unit_own = tokens.astype(jnp.float32) * inv_rms
    gain_own = lax.dynamic_slice_in_dim(
        gain, lax.axis_index(PLANE) * own_width, own_width, 0
    )
    d_unit = summed * gain_own
    row_sum, gain_part = sums(jnp.sum(unit_own * d_unit, axis=1), jnp.sum(unit_own * summed, axis=0))
    row_mean = row_sum / width
    grad_input = (
        cotangent.astype(jnp.float32) + inv_rms * (d_unit - unit_own * row_mean[:, None])
    ).astype(jnp.bfloat16)
    return grad_input, gain_part


def reduced(tokens, cotangent, gain, w_gate, w_up, w_down):
    full_x = lax.all_gather(tokens, PLANE, axis=1, tiled=True)
    full_dy = lax.all_gather(cotangent, PLANE, axis=1, tiled=True)
    inv_rms, normed = normalise(full_x, gain)
    hidden, d_gate, d_up = hidden_grads(normed, full_dy, w_gate, w_up, w_down)
    grad_down = 0.5 * left_product(hidden, full_dy)
    grad_gate = left_product(d_gate, normed)
    grad_up = left_product(d_up, normed)
    grad_input, gain_part = input_grads(
        tokens, cotangent, gain, inv_rms, hidden_sum(d_gate, d_up, w_gate, w_up),
        lambda rows_part, gain_part: (lax.psum(rows_part, PLANE), gain_part),
    )
    grad_gate, grad_up, grad_down, grad_gain = lax.psum(
        (grad_gate, grad_up, grad_down, gain_part), "rep"
    )
    return (grad_input, grad_gain, grad_gate, grad_up, grad_down)


TILE = 256
BLOCK = 64
MESH = pl.DeviceIdType.MESH
OWN, ACROSS_X, ACROSS_Y, CORNER = range(4)


def step_kernel(
    x_ref, dy_ref, gain_ref, wg_ref, wu_ref, wd_ref,
    grad_a, grad_b, grad_c, act_tail, nrm_tail, dy_tail, gi_ref, gg_ref,
    act_main, nrm_main, buf, wts, gain, inv, turned, own_part, pair_out, pair_in, own_sum, plane_out, plane_in,
    row_out, row_in, gain_out, gain_in,
    load_sem, send_sem, recv_sem, line_own, line_corner, corner_sem, pair_sem, late_sem,
    give_sem, take_sem, block_send, block_recv, row_send, row_recv, gain_send, gain_recv,
):
    z, y, t = lax.axis_index("rep"), lax.axis_index("fs"), lax.axis_index("tp")
    rows, cols = x_ref.shape
    hidden, width = wg_ref.shape
    total = 4 * rows
    half = rows // 2
    split = rows + TILE
    core = lax.rem(t, 2)
    other = 1 - 2 * core
    x_id = (z, y, lax.rem(t + 2, 4))
    y_id = (z, 1 - y, t)
    corner_id = (z, 1 - y, lax.rem(t + 2, 4))
    pair_id = (z, y, t + other)
    is_end = lax.rem(z + 1, 4) < 2
    is_mid = jnp.logical_not(is_end)
    inner_z = 1 + lax.rem(z, 2)
    inner_id = (inner_z, y, t)
    outer_id = (3 * lax.div(z, 2), y, t)
    inner_slot = 2 - lax.rem(lax.div(z + 1, 2), 2)
    column = (
        y * 4 + t,
        y * 4 + lax.rem(t + 2, 4),
        (1 - y) * 4 + t,
        (1 - y) * 4 + lax.rem(t + 2, 4),
    )
    pair_column = tuple(c + other for c in column)

    def across(col):
        return pl.ds(pl.multiple_of(col * cols, cols), cols)

    def piece(slot, col, p, start=0, size=rows):
        if isinstance(slot, int):
            window = pl.ds(slot * rows + start, size)
        else:
            window = pl.ds(pl.multiple_of(slot * rows + start, 64), size)
        return buf.at[p, window, across(col)]

    grads = (grad_a, grad_b, grad_c)
    sent = []
    numbers = {}

    def number(*key):
        return numbers.setdefault(key, len(numbers))


    def send(make, guard=None):
        if guard is None:
            make().start()
        else:
            pl.when(guard)(lambda: make().start())
        sent.append((make, () if guard is None else (guard,)))

    def remote(src, dst, ssem, rsem, target):
        return pltpu.make_async_remote_copy(
            src_ref=src, dst_ref=dst, send_sem=ssem, recv_sem=rsem,
            device_id=target, device_id_type=MESH,
        )

    def arrive(ref, sem):
        pltpu.make_async_remote_copy(
            src_ref=ref, dst_ref=ref, send_sem=send_sem.at[0], recv_sem=sem,
            device_id=pair_id, device_id_type=MESH,
        ).wait_recv()

    def move(slot, q, p, kind, lands, target, start=0, size=rows):
        own_number = number(kind, slot, p)

        def make():
            ref = piece(slot, column[q], p, start, size)
            return remote(ref, ref, send_sem.at[own_number], lands[0].at[lands[1], slot, p], target)

        send(make)

    def to_pair(slot, q, p):
        move(slot, q, p, q, (pair_sem, q), pair_id)

    def to_x(slot, p):
        move(slot, OWN, p, 4, (recv_sem, 0), x_id)

    def to_y(slot, p):
        move(slot, OWN, p, 5, (recv_sem, 1), y_id)

    def split_across(p, first):
        a, b = (0, half) if first else (half, 0)
        if first:
            move(0, OWN, p, 4, (recv_sem, 0), x_id, a, half)
            move(0, OWN, p, 5, (recv_sem, 1), y_id, b, half)
        else:
            move(0, OWN, p, 12, (late_sem, 0), x_id, a, half)
            move(0, OWN, p, 13, (late_sem, 1), y_id, b, half)

    def relay(slot, p):
        move(slot, ACROSS_X, p, 6, (corner_sem, 0), y_id, 0, half)
        move(slot, ACROSS_Y, p, 7, (corner_sem, 1), x_id, half, half)

    def along(slot, q, p, there, kind, target, guard):
        own_number = number(kind, slot, p)
        line = line_own if q == OWN else line_corner

        def make():
            return remote(
                piece(slot, column[q], p), piece(there, column[q], p),
                send_sem.at[own_number], line.at[there - 1, p], target,
            )

        send(make, guard)

    def to_inner(slot, q, p, there, guard=None):
        along(slot, q, p, there, 8 if q == OWN else 9, inner_id, guard)

    def to_outer(slot, q, p, there):
        along(slot, q, p, there, 10 if q == OWN else 11, outer_id, is_mid)

    def landed(slot, q, p):
        if q in (ACROSS_X, ACROSS_Y):
            sem = recv_sem.at[q - 1, slot, p]
        else:
            sem = (line_own if q == OWN else line_corner).at[slot - 1, p]
        arrive(piece(slot, column[q], p), sem)

    def corner_landed(slot, p):
        arrive(piece(slot, column[CORNER], p, 0, half), corner_sem.at[0, slot, p])
        arrive(piece(slot, column[CORNER], p, half, half), corner_sem.at[1, slot, p])

    def pair_landed(slot, p):
        for q in range(4):
            arrive(piece(slot, pair_column[q], p), pair_sem.at[q, slot, p])

    def onward(slot, q, p):
        if slot == 1:
            to_outer(1, q, p, 2)
        elif slot == 2:
            to_inner(2, q, p, 3, is_mid)
        else:
            to_outer(3, q, p, 3)

    def own_piece(slot, p):
        landed(slot, OWN, p)
        onward(slot, OWN, p)
        to_pair(slot, OWN, p)

    def own_across(slot, p):
        to_x(slot, p)
        to_y(slot, p)

    def split_landed(p):
        arrive(piece(0, column[ACROSS_X], p, 0, half), recv_sem.at[0, 0, p])
        arrive(piece(0, column[ACROSS_Y], p, half, half), recv_sem.at[1, 0, p])
        relay(0, p)

    def split_rest(p):
        arrive(piece(0, column[ACROSS_X], p, half, half), late_sem.at[0, 0, p])
        arrive(piece(0, column[ACROSS_Y], p, 0, half), late_sem.at[1, 0, p])
        to_pair(0, ACROSS_X, p)
        to_pair(0, ACROSS_Y, p)

    def plane_piece(slot, p):
        landed(slot, ACROSS_X, p)
        landed(slot, ACROSS_Y, p)
        if slot == 0:
            relay(0, p)
        elif slot == 1 and p == 0:
            guarded(is_end, lambda: relay(1, 0))
        to_pair(slot, ACROSS_X, p)
        to_pair(slot, ACROSS_Y, p)

    def corner_piece(slot, p):
        if slot == 0:
            corner_landed(0, p)
            to_inner(0, CORNER, p, inner_slot)
            if p == 1:
                to_outer(0, CORNER, 1, 1)
        elif slot == 1 and p == 0:
            pl.when(is_end)(lambda: corner_landed(1, p))

            def passed_on():
                landed(1, CORNER, p)
                onward(1, CORNER, p)

            guarded(is_mid, passed_on)
        else:
            landed(slot, CORNER, p)
            onward(slot, CORNER, p)
        to_pair(slot, CORNER, p)

    def guarded(guard, act_on):
        before = len(sent)

        @pl.when(guard)
        def _():
            act_on()

        for i in range(before, len(sent)):
            make, inside = sent[i]
            sent[i] = (make, (guard,) + inside)

    loads = [
        pltpu.make_async_copy(ref, piece(0, column[OWN], p), load_sem.at[p])
        for p, ref in enumerate((x_ref, dy_ref))
    ]
    loads.append(pltpu.make_async_copy(gain_ref, gain, load_sem.at[2]))
    for i, ref in enumerate((wg_ref, wu_ref, wd_ref)):
        loads.append(pltpu.make_async_copy(ref, wts.at[i], load_sem.at[3 + i]))
    for load in loads:
        load.start()

    plane_peers = []
    for k in range(1, 8):
        far_y, far_x, far_core = k // 4, (k // 2) % 2, k % 2
        peer_t = lax.rem(t + 2 * far_x, 4)
        if far_core:
            peer_t = peer_t + other
        plane_peers.append((z, lax.rem(y + far_y, 2), peer_t))
    line_peers = [(lax.rem(z + k, 4), y, t) for k in range(1, 4)]
    barrier = pltpu.get_barrier_semaphore()
    for target in plane_peers + line_peers:
        pl.semaphore_signal(barrier, inc=1, device_id=target, device_id_type=MESH)
    pl.semaphore_wait(barrier, len(plane_peers) + len(line_peers))

    def place(start):
        if start < 3 * rows:
            return act_main, nrm_main, start if start < split else start - split
        return act_tail, nrm_tail, start - 3 * rows

    def normalise_rows(start, stop):
        gain_row = gain[...]
        _, nrm, base = place(start)

        def block(i, _):
            window = pl.ds(pl.multiple_of(start + i * BLOCK, BLOCK), BLOCK)
            xf = buf[0, window, :].astype(jnp.float32)
            scale = lax.rsqrt(jnp.sum(xf * xf, axis=1, keepdims=True) / width + EPS)
            nrm[pl.ds(pl.multiple_of(base + i * BLOCK, BLOCK), BLOCK), :] = (
                xf * scale * gain_row
            ).astype(jnp.bfloat16)
            if start == 0:
                inv[window, :] = jnp.broadcast_to(scale, (BLOCK, inv.shape[1]))
            return 0

        lax.fori_loop(0, (stop - start) // BLOCK, block, 0, unroll=2)

    def hidden_rows(start, stop, hooks=()):
        hooks = hooks + (lambda: None,) * (4 - len(hooks))
        last = start == 3 * rows
        act, nrm, base = place(start)
        window = slice(base, base + stop - start)
        gate = right_product(wts[0], nrm[window, :])
        hooks[0]()
        up = right_product(wts[1], nrm[window, :])
        hooks[1]()
        if last:
            dy_tail[...] = buf[1, start:stop, :]
        d_hidden = 0.5 * right_product(wts[2], buf[1, start:stop, :])
        hooks[2]()
        sig = jax.nn.sigmoid(gate)
        active = gate * sig
        act[0, :, window] = (active * up).astype(jnp.bfloat16)
        act[1, :, window] = (d_hidden * up * sig * (1.0 + gate * (1.0 - sig))).astype(jnp.bfloat16)
        act[2, :, window] = (d_hidden * active).astype(jnp.bfloat16)
        hooks[3]()

    def weight_grads(start, stop, first, last, fresh):
        act, nrm, base = place(start)
        window = slice(base, base + stop - start)
        step = 4 * TILE if stop - start == TILE else 2 * TILE

        def tile(j, _):
            span = pl.ds(pl.multiple_of(j * step, step), step)
            for i, right in enumerate((nrm, nrm, None)):
                value = nrm[window, span] if right is not None else buf[1, start:stop, span]
                left = act[(i + 1) % 3, :, window]
                product = jnp.dot(left, value, preferred_element_type=jnp.float32)
                if i == 2:
                    product = 0.5 * product
                if fresh:
                    grads[i][:, span] = product
                else:
                    grads[i][:, span] += product
            return 0

        lax.fori_loop(first * (width // step) // 4, last * (width // step) // 4, tile, 0)

    order = (ACROSS_X, ACROSS_Y, CORNER, OWN)
    block_ids = {CORNER: corner_id, ACROSS_X: x_id, ACROSS_Y: y_id}

    def give_pair():
        for i in range(2):
            turned[i] = act_main[1 + i, :, 0:rows].T
        for k, q in enumerate(order):
            both = pl.ds(pl.multiple_of((column[q] - core) * cols, 2 * cols), 2 * cols)
            product = jnp.dot(turned[0], wts[0, :, both], preferred_element_type=jnp.float32) + jnp.dot(
                turned[1], wts[1, :, both], preferred_element_type=jnp.float32
            )

            def keep(mine, theirs, k=k):
                own_part[k] = mine
                pair_out[k] = theirs.astype(jnp.bfloat16)

            low, high = product[:, :cols], product[:, cols:]
            pl.when(core == 0)(lambda: keep(low, high))
            pl.when(core == 1)(lambda: keep(high, low))
            send(lambda k=k: remote(pair_out.at[k], pair_in.at[k], give_sem.at[k], take_sem.at[k], pair_id))

    def give_plane():
        for k, q in enumerate(order):
            arrive(pair_in.at[k], take_sem.at[k])
            product = own_part[k] + pair_in[k].astype(jnp.float32)
            if q == OWN:
                own_sum[...] = product
            else:
                plane_out[k] = product.astype(jnp.bfloat16)

    def send_plane(k):
        send(lambda: remote(
            plane_out.at[k], plane_in.at[k], block_send.at[k], block_recv.at[k], block_ids[order[k]]
        ))

    def own_values():
        unit = buf[0, 0:rows, across(column[OWN])].astype(jnp.float32) * inv[:, 0:1]
        gain_own = gain[0:1, across(column[OWN])]
        return unit, gain_own

    def take_plane():
        for k in range(3):
            arrive(plane_in.at[k], block_recv.at[k])
        summed = own_sum[...]
        for k in range(3):
            summed = summed + plane_in[k].astype(jnp.float32)
        own_sum[...] = summed
        unit, gain_own = own_values()
        product = unit * summed
        gain_out[...] = jnp.broadcast_to(jnp.sum(product, axis=0, keepdims=True), gain_out.shape)
        product = product * gain_own
        lanes = inv.shape[1]
        folded = product[:, 0:lanes]
        for i in range(1, cols // lanes):
            folded = folded + product[:, i * lanes:(i + 1) * lanes]
        row_out[...] = jnp.broadcast_to(jnp.sum(folded.T, axis=0, keepdims=True), row_out.shape)
        for k, target in enumerate(plane_peers):
            send(lambda k=k, target=target: remote(
                row_out, row_in.at[k], row_send.at[k], row_recv.at[k], target
            ))
        for k, target in enumerate(line_peers):
            send(lambda k=k, target=target: remote(
                gain_out, gain_in.at[k], gain_send.at[k], gain_recv.at[k], target
            ))

    def finish_input():
        row = row_out[0:1, :]
        for k in range(7):
            arrive(row_in.at[k], row_recv.at[k])
            row = row + row_in[k, 0:1, :]
        summed_gain = gain_out[...]
        for k in range(3):
            arrive(gain_in.at[k], gain_recv.at[k])
            summed_gain = summed_gain + gain_in[k]
        gg_ref[...] = summed_gain[0:1, :]
        lanes = inv.shape[1]
        row_mean = jnp.broadcast_to(row / width, (lanes, rows)).T
        unit, gain_own = own_values()
        d_unit = own_sum[...] * gain_own
        dy_own = buf[1, 0:rows, across(column[OWN])].astype(jnp.float32)
        gi_ref[...] = (dy_own + inv[:, 0:1] * (d_unit - unit * row_mean[:, 0:1])).astype(gi_ref.dtype)

    for p in range(2):
        loads[p].wait()
        to_inner(0, OWN, p, inner_slot)
        to_outer(0, OWN, p, 1)
        if p == 0:
            to_x(0, p)
            to_y(0, p)
        else:
            split_across(p, True)
        to_pair(0, OWN, p)
    plane_piece(0, 0)
    split_across(1, False)
    own_piece(1, 0)
    guarded(is_mid, lambda: own_piece(2, 0))
    split_landed(1)
    own_piece(1, 1)
    guarded(is_mid, lambda: own_piece(2, 1))
    corner_piece(0, 0)
    own_across(1, 0)
    own_across(1, 1)

    def middle_across():
        own_across(2, 0)
        own_across(2, 1)

    guarded(is_mid, middle_across)

    def either(at_end, at_mid):
        guarded(is_end, at_end)
        guarded(is_mid, at_mid)

    def all_of(*steps):
        def run():
            for step in steps:
                step()

        return run

    def far_own(p):
        either(lambda: own_piece(2, p), lambda: own_piece(3, p))

    def end_across():
        for p in range(2):
            guarded(is_end, lambda: own_across(2, p))

    def mid_corner(slot, p):
        guarded(is_mid, lambda: corner_piece(slot, p))

    def end_corner(slot, p):
        guarded(is_end, lambda: corner_piece(slot, p))

    loads[2].wait()
    pair_landed(0, 0)
    normalise_rows(0, rows)
    split_rest(1)
    for i in range(3):
        loads[3 + i].wait()
    hidden_rows(0, rows, (
        all_of(lambda: corner_piece(0, 1), lambda: far_own(0)),
        lambda: pair_landed(0, 1),
        lambda: mid_corner(2, 0),
        all_of(lambda: plane_piece(1, 0), lambda: far_own(1)),
    ))
    give_pair()
    mid_corner(2, 1)
    plane_piece(1, 1)
    end_across()
    weight_grads(0, rows, 0, 1, True)
    mid_corner(1, 0)
    give_plane()
    end_corner(1, 0)
    end_corner(1, 1)
    weight_grads(0, rows, 1, 3, True)
    guarded(is_end, lambda: own_piece(3, 0))
    mid_corner(1, 1)
    weight_grads(0, rows, 3, 4, True)
    send_plane(0)
    send_plane(1)
    pair_landed(1, 0)
    middle = (rows + TILE, rows + 2 * TILE, rows + 3 * TILE)
    normalise_rows(rows, middle[0])
    hidden_rows(rows, middle[0], (lambda: None, lambda: pair_landed(1, 1)))
    guarded(is_end, lambda: own_piece(3, 1))
    mid_corner(3, 0)
    plane_piece(2, 0)
    send_plane(2)
    weight_grads(rows, middle[0], 0, 2, False)
    own_across(3, 0)
    weight_grads(rows, middle[0], 2, 4, False)
    end_corner(2, 0)
    pair_landed(2, 0)
    normalise_rows(middle[0], middle[2])
    plane_piece(2, 1)
    mid_corner(3, 1)
    end_corner(2, 1)
    hidden_rows(middle[0], middle[2], (
        lambda: None,
        all_of(lambda: own_across(3, 1), lambda: pair_landed(2, 1)),
    ))
    end_corner(3, 0)
    take_plane()
    weight_grads(split, 3 * rows, 0, 3, False)
    plane_piece(3, 0)
    weight_grads(split, 3 * rows, 3, 4, False)
    end_corner(3, 1)
    pair_landed(3, 0)
    normalise_rows(3 * rows, total)
    hidden_rows(3 * rows, total, (
        lambda: plane_piece(3, 1), all_of(finish_input, lambda: pair_landed(3, 1)),
    ))
    for make, guards in sent:
        if not guards:
            make().wait_send()
        else:
            pl.when(functools.reduce(jnp.logical_and, guards))(lambda make=make: make().wait_send())


def fused_step(tokens, cotangent, gain, w_gate, w_up, w_down):
    rows, cols = tokens.shape
    hidden, width = w_gate.shape
    total = 4 * rows
    half_type, full_type = jnp.bfloat16, jnp.float32
    hbm = pl.BlockSpec(memory_space=pltpu.HBM)
    vmem = pl.BlockSpec(memory_space=pltpu.VMEM)
    dma = pltpu.SemaphoreType.DMA
    return pl.pallas_call(
        step_kernel,
        out_shape=[
            pltpu.VMEM((hidden, width), full_type),
            pltpu.VMEM((hidden, width), full_type),
            pltpu.VMEM((hidden, width), full_type),
            pltpu.VMEM((3, hidden, rows), half_type),
            pltpu.VMEM((rows, width), half_type),
            pltpu.VMEM((rows, width), half_type),
            pltpu.VMEM((rows, cols), half_type),
            pltpu.VMEM((1, cols), full_type),
        ],
        in_specs=[hbm] * 6,
        out_specs=[vmem] * 8,
        scratch_shapes=[
            pltpu.VMEM((3, hidden, rows + TILE), half_type),
            pltpu.VMEM((rows + TILE, width), half_type),
            pltpu.VMEM((2, total, width), half_type),
            pltpu.VMEM((3, hidden, width), half_type),
            pltpu.VMEM((1, width), full_type),
            pltpu.VMEM((rows, 128), full_type),
            pltpu.VMEM((2, rows, hidden), half_type),
            pltpu.VMEM((4, rows, cols), full_type),
            pltpu.VMEM((4, rows, cols), half_type),
            pltpu.VMEM((4, rows, cols), half_type),
            pltpu.VMEM((rows, cols), full_type),
            pltpu.VMEM((3, rows, cols), half_type),
            pltpu.VMEM((3, rows, cols), half_type),
            pltpu.VMEM((8, rows), full_type),
            pltpu.VMEM((7, 8, rows), full_type),
            pltpu.VMEM((8, cols), full_type),
            pltpu.VMEM((3, 8, cols), full_type),
            dma((6,)), dma((76,)), dma((2, 4, 2)), dma((3, 2)), dma((3, 2)),
            dma((2, 2, 2)), dma((4, 4, 2)), dma((2, 1, 2)),
            dma((4,)), dma((4,)), dma((3,)), dma((3,)), dma((7,)), dma((7,)), dma((3,)), dma((3,)),
        ],
        compiler_params=pltpu.CompilerParams(
            collective_id=0, has_side_effects=True, vmem_limit_bytes=37 * 2**20
        ),
        name="step",
    )(tokens, cotangent, gain.reshape(1, width), w_gate, w_up, w_down)


def last_kernel(grad_a, grad_b, grad_c, act, nrm, dy, gi, gg, gate_ref, up_ref, down_ref, gi_ref, gg_ref, stage, sem):
    width = nrm.shape[1]
    step = 2 * TILE
    grads = (grad_a, grad_b, grad_c)
    outs = (gate_ref, up_ref, down_ref)
    small = [
        pltpu.make_async_copy(gi, gi_ref, sem.at[2, 0]),
        pltpu.make_async_copy(gg, gg_ref, sem.at[2, 1]),
    ]
    for copy in small:
        copy.start()
    waiting = [[], []]
    for j in range(width // step):
        span = slice(j * step, (j + 1) * step)
        slot = j % 2
        for copy in waiting[slot]:
            copy.wait()
        waiting[slot] = []
        for i in range(3):
            left = act[(i + 1) % 3]
            value = dy[:, span] if i == 2 else nrm[:, span]
            product = jnp.dot(left, value, preferred_element_type=jnp.float32)
            if i == 2:
                product = 0.5 * product
            stage[slot, i] = grads[i][:, span] + product
            copy = pltpu.make_async_copy(stage.at[slot, i], outs[i].at[:, span], sem.at[slot, i])
            copy.start()
            waiting[slot].append(copy)
    for copy in waiting[0] + waiting[1] + small:
        copy.wait()


def fused(tokens, cotangent, gain, w_gate, w_up, w_down):
    rows, cols = tokens.shape
    hidden, width = w_gate.shape
    parts = fused_step(tokens, cotangent, gain, w_gate, w_up, w_down)
    full = jax.ShapeDtypeStruct((hidden, width), jnp.float32)
    vmem = pl.BlockSpec(memory_space=pltpu.VMEM)
    grad_gate, grad_up, grad_down, grad_input, grad_gain = pl.pallas_call(
        last_kernel,
        out_shape=[
            full, full, full,
            jax.ShapeDtypeStruct((rows, cols), tokens.dtype),
            jax.ShapeDtypeStruct((1, cols), jnp.float32),
        ],
        in_specs=[vmem] * 8,
        out_specs=[pl.BlockSpec(memory_space=pltpu.HBM)] * 5,
        scratch_shapes=[
            pltpu.VMEM((2, 3, hidden, 2 * TILE), jnp.float32),
            pltpu.SemaphoreType.DMA((3, 3)),
        ],
        compiler_params=pltpu.CompilerParams(vmem_limit_bytes=20 * 2**20),
        name="last",
    )(*parts)
    return grad_input, grad_gain[0], grad_gate, grad_up, grad_down


def fits_fused(tokens, w_gate):
    sizes = tuple(lax.axis_size(name) for name in ("rep", "fs", "tp"))
    rows, cols = tokens.shape
    hidden, width = w_gate.shape
    return (
        sizes == (4, 2, 4)
        and rows == TILE + TILE // 2
        and cols == TILE
        and width == 8 * cols
        and hidden % 16 == 0
        and 24 * hidden * width <= 34 * 2**20
    )


def gathered(tokens, cotangent, gain, w_gate, w_up, w_down):
    rows, cols = tokens.shape
    reps, plane = lax.axis_size("rep"), lax.axis_size(PLANE)
    both = lax.all_gather(jnp.stack([tokens, cotangent]), ("rep",) + PLANE)
    both = both.reshape(reps, plane, 2, rows, cols).transpose(2, 0, 3, 1, 4)
    both = both.reshape(2, reps * rows, plane * cols)
    inv_rms, normed = normalise(both[0], gain)
    dy = both[1]
    hidden, d_gate, d_up = hidden_grads(normed, dy, w_gate, w_up, w_down)
    start = lax.axis_index("rep") * rows
    own = lambda a: lax.dynamic_slice_in_dim(a, start, rows, 0)
    partial_value = hidden_sum(own(d_gate), own(d_up), w_gate, w_up).astype(jnp.bfloat16)
    partial_value, hidden, d_gate, d_up = lax.optimization_barrier(
        (partial_value, hidden, d_gate, d_up)
    )
    grad_input, grad_gain = input_grads(
        tokens, cotangent, gain, own(inv_rms), partial_value, axis_sums
    )
    grad_down = 0.5 * left_product(hidden, dy)
    grad_gate = left_product(d_gate, normed)
    grad_up = left_product(d_up, normed)
    return (grad_input, grad_gain, grad_gate, grad_up, grad_down)


def local(tokens, cotangent, gain, w_gate, w_up, w_down):
    reps = lax.axis_size("rep")
    token_bytes = 2 * 2 * tokens.shape[0] * reps * w_gate.shape[1]
    grad_bytes = 3 * 4 * w_gate.size
    plan = gathered if token_bytes < grad_bytes else reduced
    if fits_fused(tokens, w_gate):
        plan = fused
    return plan(tokens, cotangent, gain, w_gate, w_up, w_down)


def solution(mesh):
    placed = (
        P("rep", PLANE),
        P("rep", PLANE),
        P(),
        P(PLANE, None),
        P(PLANE, None),
        P(PLANE, None),
    )
    return jax.shard_map(
        local,
        mesh=mesh,
        in_specs=placed,
        out_specs=(
            P("rep", PLANE),
            P(PLANE),
            P(PLANE, None),
            P(PLANE, None),
            P(PLANE, None),
        ),
        check_vma=False,
    )
```
